32 devices in a mesh: dp: 4 (over y, x), kv: 4 (over z), tp: 2 (over core).
Axes of the slice: x: 2, y: 2, z: 4, core: 2. Of those that a mesh axis runs over, the one named last changes fastest.
Arguments:
- tokens: bfloat16 [1024, 4096], P('dp', ('kv', 'tp')), may hold values from -53 to 53
- carried_state: float32 [1024, 16, 128, 128], P(('dp', 'kv', 'tp')), may hold values from -9 to 9
- first_gain: float32 [4096], replicated, may hold values from 0.1 to 1.9
- first_gate: bfloat16 [4096, 11264], P(None, ('kv', 'tp')), may hold values from -0.09375 to 0.09375
- first_up: bfloat16 [4096, 11264], P(None, ('kv', 'tp')), may hold values from -0.09375 to 0.09375
- first_down: bfloat16 [11264, 4096], P(('kv', 'tp')), may hold values from -0.078125 to 0.078125
- mix_gain: float32 [4096], replicated, may hold values from 0.1 to 1.9
- query_weight: bfloat16 [4096, 2048], P(('kv', 'tp')), may hold values from -0.09375 to 0.09375
- forget_weight: bfloat16 [4096, 2048], P(('kv', 'tp')), may hold values from -0.09375 to 0.09375
- input_weight: bfloat16 [4096, 2048], P(('kv', 'tp')), may hold values from -0.09375 to 0.09375
- outgate_weight: bfloat16 [4096, 2048], P(('kv', 'tp')), may hold values from -0.09375 to 0.09375
- forget_floor: float32 [2048], replicated, may hold values from 0.05 to 0.9
- head_gain: float32 [128], replicated, may hold values from 0.1 to 1.9
- output_weight: bfloat16 [2048, 4096], P(None, ('kv', 'tp')), may hold values from -0.125 to 0.125
- second_gain: float32 [4096], replicated, may hold values from 0.1 to 1.9
- second_gate: bfloat16 [4096, 11264], P(None, ('kv', 'tp')), may hold values from -0.09375 to 0.09375
- second_up: bfloat16 [4096, 11264], P(None, ('kv', 'tp')), may hold values from -0.09375 to 0.09375
- second_down: bfloat16 [11264, 4096], P(('kv', 'tp')), may hold values from -0.078125 to 0.078125
Outputs:
- layer_out: bfloat16 [1024, 4096], P('dp', ('kv', 'tp'))
- next_state: float32 [1024, 16, 128, 128], P(('dp', 'kv', 'tp'))
The draws below stay inside these ranges and needn't reach their ends.
All inputs are finite; a program needn't handle non-finite values.
Results may differ from the reference program's by a relative error of at most 0.018.
Values may be sent and summed in bfloat16 or wider, within the bound.
A program may use at most 256 MiB of HBM per device.

```python
import jax
import jax.numpy as jnp
from jax import lax

D = 4096
FF = 11264
HEADS = 16
KEY = 128
VAL = 128
SEQS = 1024
KW = 2048
VW = 2048


def draw_tokens(key, part):
    keys = jax.random.split(jax.random.fold_in(key, 11), 3)
    row_scale = jnp.exp(jax.random.uniform(keys[0], (SEQS, 1), jnp.float32, jnp.log(0.3), jnp.log(3.0)))
    col_trend = jnp.exp(jnp.linspace(jnp.log(0.4), jnp.log(2.5), D)).astype(jnp.float32).reshape(1, D)
    rough = jax.random.uniform(keys[1], (1, D), jnp.float32, 0.6, 1.4)
    base = jnp.clip(jax.random.normal(keys[2], (SEQS, D), jnp.float32), -5.0, 5.0)
    return (base * rough * col_trend * row_scale).astype(jnp.bfloat16)


def strengthened(result, rng, source, target, shards_of, factor):
    owner, partner = [(jnp.arange(result.shape[axis_at]) // (result.shape[axis_at] // shards_of)).reshape([-1 if axis == axis_at else 1 for axis in range(result.ndim)]) for axis_at in (source, target)]
    chosen = jax.random.permutation(rng, shards_of)[partner]
    strong = (owner == chosen) | (owner == (partner + shards_of // 2) % shards_of)
    return jnp.where(strong, factor * result, result)


def block_scale(stream_key, shape, cuts, least, top_value):
    loudness = 1.0
    for dim, parts in cuts:
        heights = jax.random.uniform(jax.random.fold_in(jax.random.fold_in(stream_key, 6), dim), (parts,), jnp.float32, least / len(cuts), top_value / len(cuts))
        loudness = loudness * jnp.repeat(jnp.exp(heights), shape[dim] // parts).reshape((-1,) + (1,) * (len(shape) - 1 - dim))
    return loudness


def scatter_about(rng, shape, width, limit, cuts=(), dtype=jnp.bfloat16):
    values = width * jax.random.normal(rng, shape, jnp.float32)
    if cuts:
        values = values * block_scale(rng, shape, cuts, -0.22, 0.18)
    return jnp.clip(values, -limit, limit).astype(dtype)


def noise_with(rng, extent, spread, most, cuts, heavy, kind=jnp.bfloat16):
    values = spread * jax.random.normal(rng, extent, jnp.float32)
    if cuts:
        values = values * block_scale(rng, extent, cuts, -0.22, 0.18)
    return jnp.clip(strengthened(values, jax.random.fold_in(rng, 3), *heavy), -most, most).astype(kind)


def setup_inputs(seed: int = 0) -> dict:
    arg_keys = jax.random.split(jax.random.key(seed), 19)
    tokens = draw_tokens(jax.random.fold_in(arg_keys[18], 71), 0)
    carried_state = scatter_about(arg_keys[1], (SEQS, HEADS, KEY, VAL), 1.5, 9.0, ((0, 32),), jnp.float32)
    first_gain = jnp.clip(1.0 + 0.18 * jax.random.normal(arg_keys[2], (D,), jnp.float32), 0.1, 1.9)
    first_gate = scatter_about(arg_keys[3], (D, FF), D ** -0.5, 0.09375, ((1, 8),))
    first_up = scatter_about(arg_keys[4], (D, FF), D ** -0.5, 0.09375, ((1, 8),))
    first_down = noise_with(arg_keys[5], (FF, D), FF ** -0.5, 0.078125, ((0, 8),), (0, 1, 8, 2.0))
    mix_gain = jnp.clip(1.0 + 0.18 * jax.random.normal(arg_keys[6], (D,), jnp.float32), 0.1, 1.9)
    query_weight = scatter_about(arg_keys[7], (D, KW), D ** -0.5, 0.09375, ((0, 8),))
    forget_weight = scatter_about(arg_keys[8], (D, KW), D ** -0.5, 0.09375, ((0, 8),))
    input_weight = scatter_about(arg_keys[9], (D, VW), D ** -0.5, 0.09375, ((0, 8),))
    outgate_weight = scatter_about(arg_keys[10], (D, VW), D ** -0.5, 0.09375, ((0, 8),))
    forget_floor = jnp.clip(jax.random.uniform(arg_keys[11], (KW,), jnp.float32, 0.05, 0.9), 0.05, 0.9)
    head_gain = jnp.clip(1.0 + 0.18 * jax.random.normal(arg_keys[12], (VAL,), jnp.float32), 0.1, 1.9)
    output_weight = scatter_about(arg_keys[13], (VW, D), VW ** -0.5, 0.125, ((1, 8),))
    second_gain = jnp.clip(1.0 + 0.18 * jax.random.normal(arg_keys[14], (D,), jnp.float32), 0.1, 1.9)
    second_gate = scatter_about(arg_keys[15], (D, FF), D ** -0.5, 0.09375, ((1, 8),))
    second_up = scatter_about(arg_keys[16], (D, FF), D ** -0.5, 0.09375, ((1, 8),))
    second_down = noise_with(arg_keys[17], (FF, D), FF ** -0.5, 0.078125, ((0, 8),), (0, 1, 8, 2.0))
    return {"tokens": tokens, "carried_state": carried_state, "first_gain": first_gain, "first_gate": first_gate, "first_up": first_up, "first_down": first_down, "mix_gain": mix_gain, "query_weight": query_weight, "forget_weight": forget_weight, "input_weight": input_weight, "outgate_weight": outgate_weight, "forget_floor": forget_floor, "head_gain": head_gain, "output_weight": output_weight, "second_gain": second_gain, "second_gate": second_gate, "second_up": second_up, "second_down": second_down}


epsilon = 1e-06

def inverse_rms(entries):
    return lax.rsqrt(lax.optimization_barrier(jnp.mean(entries * entries, axis=-1, keepdims=True)) + epsilon)

def half_channel(inputs, gain_vec, gate_weight, up_weight, down_weight):
    widened = inputs.astype(jnp.float32)
    row_scale = inverse_rms(widened)
    scaled = (widened * gain_vec).astype(jnp.bfloat16)
    gate_acc = row_scale * jnp.dot(scaled, gate_weight, preferred_element_type=jnp.float32)
    up_acc = row_scale * jnp.dot(scaled, up_weight, preferred_element_type=jnp.float32)
    hidden = (jax.nn.silu(gate_acc) * up_acc).astype(jnp.bfloat16)
    return (widened + 0.5 * jnp.dot(hidden, down_weight, preferred_element_type=jnp.float32)).astype(jnp.bfloat16)

def reference(tokens, carried_state, first_gain, first_gate, first_up, first_down, mix_gain, query_weight, forget_weight, input_weight, outgate_weight, forget_floor, head_gain, output_weight, second_gain, second_gate, second_up, second_down):
    mixer_in = half_channel(tokens, first_gain, first_gate, first_up, first_down)
    widened = mixer_in.astype(jnp.float32)
    row_scale = inverse_rms(widened)
    scaled = (widened * mix_gain).astype(jnp.bfloat16)
    seq_count = tokens.shape[0]
    query_act = (row_scale * jnp.dot(scaled, query_weight, preferred_element_type=jnp.float32)).reshape(seq_count, HEADS, KEY)
    forget_pre = (row_scale * jnp.dot(scaled, forget_weight, preferred_element_type=jnp.float32)).reshape(seq_count, HEADS, KEY)
    input_val = (row_scale * jnp.dot(scaled, input_weight, preferred_element_type=jnp.float32)).reshape(seq_count, HEADS, VAL)
    gate_pre = (row_scale * jnp.dot(scaled, outgate_weight, preferred_element_type=jnp.float32)).reshape(seq_count, HEADS, VAL)
    floor_grid = forget_floor.reshape(HEADS, KEY)
    forget = floor_grid + (1.0 - floor_grid) * jax.nn.sigmoid(forget_pre)
    next_state = forget[..., None] * carried_state + (1.0 - forget)[..., None] * input_val[:, :, None, :]
    readout = lax.optimization_barrier(jnp.sum(next_state * jax.nn.silu(query_act)[..., None], axis=2))
    normed = readout * inverse_rms(readout) * head_gain
    mixer_out = (normed * jax.nn.silu(gate_pre)).reshape(seq_count, VW).astype(jnp.bfloat16)
    middle = (widened + jnp.dot(mixer_out, output_weight, preferred_element_type=jnp.float32)).astype(jnp.bfloat16)
    layer_out = half_channel(middle, second_gain, second_gate, second_up, second_down)
    return (layer_out, next_state)
```

```python
import functools

import jax
import jax.numpy as jnp
from jax import lax
from jax.experimental import pallas as pl
from jax.experimental.pallas import tpu as pltpu
from jax.sharding import PartitionSpec as P

epsilon = 1e-06
MESH = pl.DeviceIdType.MESH
VMEM_LIMIT = 63 * 1024 * 1024
LANES = 128


def remote(src, dst, send_sem, recv_sem, kv, tp):
    return pltpu.make_async_remote_copy(
        src_ref=src,
        dst_ref=dst,
        send_sem=send_sem,
        recv_sem=recv_sem,
        device_id={"kv": kv, "tp": tp},
        device_id_type=MESH,
    )


def greet_all(me, core, chips):
    barrier = pltpu.get_barrier_semaphore()
    pl.semaphore_signal(
        barrier, inc=1, device_id={"kv": me, "tp": 1 - core}, device_id_type=MESH
    )
    for step in range(1, chips):
        pl.semaphore_signal(
            barrier,
            inc=1,
            device_id={"kv": lax.rem(me + step, chips), "tp": core},
            device_id_type=MESH,
        )
    pl.semaphore_wait(barrier, chips)


def greet_chain(me, core, chips):
    barrier = pltpu.get_barrier_semaphore()
    pl.semaphore_signal(
        barrier, inc=1, device_id={"kv": me, "tp": 1 - core}, device_id_type=MESH
    )

    @pl.when(me > 0)
    def _():
        pl.semaphore_signal(
            barrier, inc=1, device_id={"kv": me - 1, "tp": core}, device_id_type=MESH
        )

    @pl.when(me < chips - 1)
    def _():
        pl.semaphore_signal(
            barrier, inc=1, device_id={"kv": me + 1, "tp": core}, device_id_type=MESH
        )

    ends = jnp.where(me > 0, 1, 0) + jnp.where(me < chips - 1, 1, 0)
    pl.semaphore_wait(barrier, 1 + ends)


def block_kernel(
    chips,
    own_ref,
    gain_ref,
    gate_hbm,
    up_hbm,
    down_hbm,
    out_ref,
    gate_w,
    up_w,
    down_w,
    cols,
    gate_acc,
    up_acc,
    squares,
    hidden,
    held,
    sib_out,
    sib_in,
    chip_out,
    chip_in,
    gate_sem,
    up_sem,
    down_sem,
    local_sem,
    fwd_send,
    pass_send,
    recv_sem,
    sib_send,
    sib_recv,
    chip_send,
    chip_recv,
):
    me = lax.axis_index("kv")
    core = lax.axis_index("tp")
    mine = me * 2 + core
    last = chips - 1
    rows, width = own_ref.shape
    full_width = width * chips * 2
    half = rows // 2
    subs = (0, 1)

    def piece(sub):
        return pl.ds(sub * half, half)

    def gate_copy(j):
        at = pl.ds(pl.multiple_of(j * width, width), width)
        return pltpu.make_async_copy(gate_hbm.at[at, :], gate_w.at[j], gate_sem.at[j])

    def up_copy(j):
        at = pl.ds(pl.multiple_of(j * width, width), width)
        return pltpu.make_async_copy(up_hbm.at[at, :], up_w.at[j], up_sem.at[j])

    def down_copy(j):
        at = pl.ds(pl.multiple_of(j * width, width), width)
        return pltpu.make_async_copy(down_hbm.at[:, at], down_w.at[j], down_sem.at[j])

    local = pltpu.make_async_copy(own_ref, cols.at[mine], local_sem)
    local.start()

    def reach(step, side):
        j = me + step * (2 * side - 1)
        fits = jnp.logical_and(j >= 0, j < chips)
        return j, jnp.logical_and(fits, jnp.logical_or(step > 0, side == 0))

    def each_block(body):
        @pl.loop(0, chips)
        def _(step):
            @pl.loop(0, 4)
            def _(i):
                j, valid = reach(step, lax.rem(i, 2))
                other = lax.div(i, 2)

                @pl.when(valid)
                def _():
                    body(j * 2 + lax.rem(core + other, 2))

    def start_in(slot):
        gate_copy(slot).start()
        up_copy(slot).start()

    each_block(start_in)
    greet_chain(me, core, chips)

    def own_copy(to, tp, sem, sub):
        at = piece(sub)
        return remote(
            own_ref.at[at], cols.at[mine, at], sem, recv_sem.at[mine, sub], to, tp
        )

    def right_copy(sub):
        return own_copy(me + 1, core, fwd_send.at[me, sub], sub)

    def left_copy(sub):
        return own_copy(me - 1, core, fwd_send.at[chips, sub], sub)

    def own_pass(sub):
        return own_copy(me, 1 - core, pass_send.at[me, sub], sub)

    def slot_copy(slot, sub, sem, to, tp):
        at = piece(sub)
        return remote(
            cols.at[slot, at], cols.at[slot, at], sem, recv_sem.at[slot, sub], to, tp
        )

    def fwd_copy(j, sub):
        to = jnp.where(j < me, me + 1, me - 1)
        return slot_copy(j * 2 + core, sub, fwd_send.at[j, sub], to, core)

    def pass_copy(j, sub):
        return slot_copy(j * 2 + core, sub, pass_send.at[j, sub], me, 1 - core)

    def forwards(j):
        return jnp.logical_or(
            jnp.logical_and(j < me, me < last), jnp.logical_and(j > me, me > 0)
        )

    for sub in subs:

        @pl.when(me < last)
        def _():
            right_copy(sub).start()

        @pl.when(me > 0)
        def _():
            left_copy(sub).start()

    for sub in subs:
        own_pass(sub).start()

    def start_down(q):
        down_copy(q * 2 + 1 - core).start()
        down_copy(q * 2 + core).start()

    def far_first(body):
        @pl.loop(0, chips)
        def _(turn):
            @pl.loop(0, 2)
            def _(side):
                q, valid = reach(last - turn, side)

                @pl.when(valid)
                def _():
                    body(q)

    far_first(start_down)

    gate_acc[...] = jnp.zeros_like(gate_acc)
    up_acc[...] = jnp.zeros_like(up_acc)
    squares[...] = jnp.zeros_like(squares)
    local.wait()

    def take(j):
        block = cols[j].astype(jnp.float32)
        squares[...] += jnp.sum(block * block, axis=1, keepdims=True)
        scaled = (block * gain_ref[j]).astype(jnp.bfloat16)
        gate_copy(j).wait()
        gate_acc[...] += jnp.dot(scaled, gate_w[j], preferred_element_type=jnp.float32)
        up_copy(j).wait()
        up_acc[...] += jnp.dot(scaled, up_w[j], preferred_element_type=jnp.float32)

    @pl.loop(0, chips)
    def _(step):
        @pl.when(step > 0)
        def _():
            for sub in subs:
                for side in (0, 1):
                    j, valid = reach(step, side)

                    @pl.when(valid)
                    def _():
                        pass_copy(j, sub).wait_recv()

                        @pl.when(forwards(j))
                        def _():
                            fwd_copy(j, sub).start()

                        pass_copy(j, sub).start()

        @pl.loop(0, 4)
        def _(i):
            j, valid = reach(step, lax.rem(i, 2))
            other = lax.div(i, 2)
            slot = j * 2 + lax.rem(core + other, 2)

            @pl.when(valid)
            def _():
                @pl.when(other == 1)
                def _():
                    for sub in subs:
                        slot_copy(slot, sub, fwd_send.at[0, 0], me, 1 - core).wait_recv()

                take(slot)

    tile = 32

    @pl.loop(0, rows // tile)
    def _(i):
        at = pl.ds(pl.multiple_of(i * tile, tile), tile)
        row_scale = lax.rsqrt(squares[at, :] / full_width + epsilon)
        gate = row_scale * gate_acc[at, :]
        hidden[at, :] = (gate * jax.nn.sigmoid(gate) * (row_scale * up_acc[at, :])).astype(
            jnp.bfloat16
        )

    def branch(j):
        down_copy(j).wait()
        return 0.5 * jnp.dot(hidden[...], down_w[j], preferred_element_type=jnp.float32)

    def sib_copy(q):
        return remote(
            sib_out.at[q], sib_in.at[q], sib_send.at[q], sib_recv.at[q], me, 1 - core
        )

    def chain_copy(q, sub):
        at = piece(sub)
        to = jnp.where(q > me, me + 1, me - 1)
        slot = jnp.where(q == me - 1, chips, q)
        return remote(
            chip_out.at[q, at],
            chip_in.at[slot, at],
            chip_send.at[q, sub],
            chip_recv.at[slot, sub],
            to,
            core,
        )

    def arrived(slot, sub):
        at = piece(sub)
        remote(
            chip_in.at[slot, at],
            chip_in.at[slot, at],
            chip_send.at[0, sub],
            chip_recv.at[slot, sub],
            me,
            1 - core,
        ).wait_recv()

    def produce(q):
        sib_out[q] = branch(q * 2 + 1 - core).astype(jnp.bfloat16)
        sib_copy(q).start()
        held[q] = branch(q * 2 + core)
        first = jnp.logical_or(
            jnp.logical_and(q > me, me == 0), jnp.logical_and(q < me, me == last)
        )

        @pl.when(first)
        def _():
            sib_copy(q).wait_recv()
            for sub in subs:
                at = piece(sub)
                chip_out[q, at] = (held[q, at] + sib_in[q, at].astype(jnp.float32)).astype(
                    jnp.bfloat16
                )
                chain_copy(q, sub).start()

    far_first(produce)

    near = jnp.where(me <= last - me, 0, 1)

    @pl.loop(1, chips - 1)
    def _(turn):
        for sub in subs:

            @pl.loop(0, 2)
            def _(i):
                leftward = lax.rem(i + near, 2)
                q = jnp.where(leftward == 1, turn - (last - me), last - (turn - me))
                goes_right = jnp.logical_and(
                    jnp.logical_and(leftward == 0, me > 0),
                    jnp.logical_and(q > me, q < chips),
                )
                goes_left = jnp.logical_and(
                    jnp.logical_and(leftward == 1, me < last),
                    jnp.logical_and(q >= 0, q < me),
                )

                @pl.when(jnp.logical_or(goes_right, goes_left))
                def _():
                    if sub == 0:
                        sib_copy(q).wait_recv()
                    arrived(q, sub)
                    at = piece(sub)
                    chip_out[q, at] = (
                        held[q, at]
                        + sib_in[q, at].astype(jnp.float32)
                        + chip_in[q, at].astype(jnp.float32)
                    ).astype(jnp.bfloat16)
                    chain_copy(q, sub).start()

    sib_copy(me).wait_recv()
    for sub in subs:
        at = piece(sub)
        held[me, at] += sib_in[me, at].astype(jnp.float32)

        @pl.when(me > 0)
        def _():
            arrived(me, sub)
            held[me, at] += chip_in[me, at].astype(jnp.float32)

        @pl.when(me < last)
        def _():
            arrived(chips, sub)
            held[me, at] += chip_in[chips, at].astype(jnp.float32)

        out_ref[at] = (held[me, at] + own_ref[at].astype(jnp.float32)).astype(out_ref.dtype)

    for sub in subs:

        @pl.when(me < last)
        def _():
            right_copy(sub).wait_send()

        @pl.when(me > 0)
        def _():
            left_copy(sub).wait_send()

    @pl.loop(0, chips)
    def _(j):
        sib_copy(j).wait_send()
        for sub in subs:
            pass_copy(j, sub).wait_send()

            @pl.when(forwards(j))
            def _():
                fwd_copy(j, sub).wait_send()

            @pl.when(j != me)
            def _():
                chain_copy(j, sub).wait_send()


def feed_forward(own, gain, gate, up, down, chips, collective_id):
    rows, width = own.shape
    units = gate.shape[1]
    blocks = chips * 2
    dma = pltpu.SemaphoreType.DMA
    half_rounds = (chips, rows, width)
    return pl.pallas_call(
        functools.partial(block_kernel, chips),
        out_shape=jax.ShapeDtypeStruct((rows, width), jnp.bfloat16),
        in_specs=[pl.BlockSpec(memory_space=pltpu.VMEM)] * 2
        + [pl.BlockSpec(memory_space=pl.ANY)] * 3,
        out_specs=pl.BlockSpec(memory_space=pltpu.VMEM),
        scratch_shapes=[
            pltpu.VMEM((blocks, width, units), jnp.bfloat16),
            pltpu.VMEM((blocks, width, units), jnp.bfloat16),
            pltpu.VMEM((blocks, units, width), jnp.bfloat16),
            pltpu.VMEM((blocks, rows, width), jnp.bfloat16),
            pltpu.VMEM((rows, units), jnp.float32),
            pltpu.VMEM((rows, units), jnp.float32),
            pltpu.VMEM((rows, 1), jnp.float32),
            pltpu.VMEM((rows, units), jnp.bfloat16),
            pltpu.VMEM(half_rounds, jnp.float32),
            pltpu.VMEM(half_rounds, jnp.bfloat16),
            pltpu.VMEM(half_rounds, jnp.bfloat16),
            pltpu.VMEM(half_rounds, jnp.bfloat16),
            pltpu.VMEM((chips + 1, rows, width), jnp.bfloat16),
            dma((blocks,)),
            dma((blocks,)),
            dma((blocks,)),
            dma,
            dma((chips + 1, 2)),
            dma((chips, 2)),
            dma((blocks, 2)),
            dma((chips,)),
            dma((chips,)),
            dma((chips, 2)),
            dma((chips + 1, 2)),
        ],
        compiler_params=pltpu.CompilerParams(
            collective_id=collective_id, has_side_effects=True, vmem_limit_bytes=VMEM_LIMIT
        ),
    )(own, gain.reshape(blocks, 1, width), gate, up, down)


def picker():
    row = lax.broadcasted_iota(jnp.int32, (16, 8 * LANES), 0)
    col = lax.broadcasted_iota(jnp.int32, (16, 8 * LANES), 1)
    return (lax.rem(row, 8) == lax.div(col, LANES)).astype(jnp.bfloat16)


def spread(eight, pick):
    high = eight.astype(jnp.bfloat16).astype(jnp.float32)
    both = jnp.concatenate([high, eight - high], axis=0).astype(jnp.bfloat16)
    return lax.dot_general(
        both, pick, (((0,), (0,)), ((), ())), preferred_element_type=jnp.float32
    )


def encode(total):
    lane = lax.broadcasted_iota(jnp.int32, (total.shape[0], LANES), 1)
    high = total.astype(jnp.bfloat16).astype(jnp.float32)
    return jnp.where(lane < LANES // 2, high, total - high)


def decode(pairs):
    return jnp.sum(pairs, axis=1, keepdims=True) * (2.0 / LANES)


def mixer_kernel(
    chips,
    pieces,
    own_ref,
    gain_ref,
    floor_ref,
    head_ref,
    query_hbm,
    forget_hbm,
    input_hbm,
    outgate_hbm,
    output_hbm,
    state_hbm,
    middle_ref,
    forget_ref,
    value_ref,
    weights,
    out_w,
    state,
    scaled,
    part,
    sib_in,
    chip_out,
    chip_in,
    total,
    scale,
    pick,
    mass,
    readout,
    mix_own,
    mixed,
    update,
    weight_sem,
    out_sem,
    state_sem,
    sib_send,
    sib_recv,
    chip_send,
    chip_recv,
    mix_send,
    pass_send,
    mix_recv,
):
    me = lax.axis_index("kv")
    core = lax.axis_index("tp")
    mine = me * 2 + core
    last = chips - 1
    rows, width = own_ref.shape
    full_width = width * chips * 2
    blocks = chips * 2
    seqs = rows // blocks
    span = weights.shape[3]
    heads = state.shape[2]
    main = 4 * span
    projections = (query_hbm, forget_hbm, input_hbm, outgate_hbm)

    def weight_copy(c, p):
        at = pl.ds(pl.multiple_of(c * span, span), span)
        return pltpu.make_async_copy(
            projections[p].at[:, at], weights.at[c, p], weight_sem.at[c, p]
        )

    def state_copy(c):
        return pltpu.make_async_copy(
            state_hbm.at[:, pl.ds(c * heads, heads)], state.at[c], state_sem.at[c]
        )

    out_copy = pltpu.make_async_copy(output_hbm, out_w, out_sem)

    @pl.loop(0, pieces)
    def _(c):
        for p in range(4):
            weight_copy(c, p).start()

    @pl.loop(0, pieces)
    def _(c):
        state_copy(c).start()

    out_copy.start()
    wide = own_ref[...].astype(jnp.float32)
    scaled[...] = (wide * gain_ref[mine]).astype(jnp.bfloat16)
    part[0, :, :, main:] = (
        encode(jnp.sum(wide * wide, axis=1, keepdims=True))
        .reshape(blocks, seqs, LANES)
        .astype(jnp.bfloat16)
    )
    pick[...] = picker()
    update[...] = wide
    greet_all(me, core, chips)

    def for_width(c, body):
        @pl.when(c == 0)
        def _():
            body(main + LANES)

        @pl.when(c > 0)
        def _():
            body(main)

    def sib_copy(c, q, size):
        at = pl.ds(0, size)
        return remote(
            part.at[c, q * 2 + 1 - core, :, at],
            sib_in.at[c, q, :, at],
            sib_send.at[c, q],
            sib_recv.at[c, q],
            me,
            1 - core,
        )

    def chain_copy(c, q, size):
        at = pl.ds(0, size)
        to = jnp.where(q > me, me + 1, me - 1)
        slot = jnp.where(q == me - 1, chips, q)
        return remote(
            chip_out.at[c, q, :, at],
            chip_in.at[c, slot, :, at],
            chip_send.at[c, q],
            chip_recv.at[c, slot],
            to,
            core,
        )

    def arrived(c, slot, size):
        at = pl.ds(0, size)
        remote(
            chip_in.at[c, slot, :, at],
            chip_in.at[c, slot, :, at],
            chip_send.at[c, 0],
            chip_recv.at[c, slot],
            me,
            1 - core,
        ).wait_recv()

    def local_sum(c, q, at):
        return part[c, q * 2 + core, :, at].astype(jnp.float32) + sib_in[c, q, :, at].astype(
            jnp.float32
        )

    def pass_on(c, q, upstream):
        def body(size):
            sib_copy(c, q, size).wait_recv()
            if upstream:
                arrived(c, q, size)

            def summed(at):
                here = local_sum(c, q, at)
                if upstream:
                    here = here + chip_in[c, q, :, at].astype(jnp.float32)
                return here

            chip_out[c, q, :, :main] = summed(slice(0, main)).astype(jnp.bfloat16)
            if size > main:
                at = slice(main, main + LANES)
                chip_out[c, q, :, at] = encode(decode(summed(at))).astype(jnp.bfloat16)
            chain_copy(c, q, size).start()

        for_width(c, body)

    @pl.loop(0, pieces)
    def _(c):
        for p in range(4):
            weight_copy(c, p).wait()
            part[c, :, :, p * span : (p + 1) * span] = (
                jnp.dot(scaled[...], weights[c, p], preferred_element_type=jnp.float32)
                .reshape(blocks, seqs, span)
                .astype(jnp.bfloat16)
            )

        @pl.loop(0, chips)
        def _(turn):
            q = jnp.where(me * 2 < chips, last - turn, turn)
            for_width(c, lambda size: sib_copy(c, q, size).start())

        @pl.loop(0, chips - 1)
        def _(turn):
            @pl.when(me == 0)
            def _():
                pass_on(c, last - turn, False)

            @pl.when(me == last)
            def _():
                pass_on(c, turn, False)

    near = jnp.where(me <= last - me, 0, 1)

    def mix_copy(c, to):
        return remote(
            mix_own.at[c],
            mixed.at[c, mine],
            mix_send.at[c, to],
            mix_recv.at[c, mine],
            to,
            core,
        )

    def own_pass(c):
        return remote(
            mix_own.at[c],
            mixed.at[c, mine],
            mix_send.at[c, me],
            mix_recv.at[c, mine],
            me,
            1 - core,
        )

    def pass_copy(c, slot, sem):
        return remote(
            mixed.at[c, slot], mixed.at[c, slot], sem, mix_recv.at[c, slot], me, 1 - core
        )

    def finish(c):
        def gather_total(size):
            sib_copy(c, me, size).wait_recv()
            at = slice(0, size)
            total[:, at] = local_sum(c, me, at)

            @pl.when(me > 0)
            def _():
                arrived(c, me, size)
                total[:, at] += chip_in[c, me, :, at].astype(jnp.float32)

            @pl.when(me < last)
            def _():
                arrived(c, chips, size)
                total[:, at] += chip_in[c, chips, :, at].astype(jnp.float32)

        for_width(c, gather_total)

        @pl.when(c == 0)
        def _():
            squares = decode(total[:, main : main + LANES])
            scale[...] = jnp.broadcast_to(
                lax.rsqrt(squares / full_width + epsilon), scale.shape
            )

        row_scale = scale[:, 0:1]
        query = row_scale * total[:, 0:span]
        query = query * jax.nn.sigmoid(query)
        floor = floor_ref[c]
        forget = floor + (1.0 - floor) * jax.nn.sigmoid(row_scale * total[:, span : 2 * span])
        value = row_scale * total[:, 2 * span : 3 * span]
        forget_ref[c] = forget
        value_ref[c] = value
        mass[...] = query * forget
        rest = query - query * forget
        state_copy(c).wait()

        @pl.loop(0, seqs // 8)
        def _(octet):
            at = pl.ds(pl.multiple_of(octet * 8, 8), 8)
            for h in range(heads):
                lanes = slice(h * LANES, (h + 1) * LANES)
                wide_mass = spread(mass[at, lanes], pick[...])
                lines = []
                for i in range(8):
                    old = state[c, octet * 8 + i, h]
                    lines.append(
                        jnp.sum(
                            old * wide_mass[:, i * LANES : (i + 1) * LANES],
                            axis=0,
                            keepdims=True,
                        )
                    )
                readout[at, lanes] = jnp.concatenate(lines, axis=0)

        gate = row_scale * total[:, 3 * span : 4 * span]
        gate = gate * jax.nn.sigmoid(gate)
        for h in range(heads):
            lanes = slice(h * LANES, (h + 1) * LANES)
            read = readout[:, lanes] + value[:, lanes] * jnp.sum(
                rest[:, lanes], axis=1, keepdims=True
            )
            read = (
                read
                * lax.rsqrt(jnp.mean(read * read, axis=1, keepdims=True) + epsilon)
                * head_ref[...]
                * gate[:, lanes]
            )
            mix_own[c, :, lanes] = read.astype(jnp.bfloat16)

        @pl.loop(1, chips)
        def _(step):
            mix_copy(c, lax.rem(me + step, chips)).start()

        own_pass(c).start()
        mixed[c, mine] = mix_own[c]

    def gather(c):
        @pl.loop(1, chips)
        def _(step):
            q = lax.rem(me + step, chips)
            pass_copy(c, q * 2 + core, mix_send.at[c, 0]).wait_recv()
            pass_copy(c, q * 2 + core, pass_send.at[c, q]).start()

        @pl.loop(0, chips)
        def _(q):
            pass_copy(c, q * 2 + 1 - core, mix_send.at[c, 0]).wait_recv()

        @pl.when(c == 0)
        def _():
            out_copy.wait()

        every = mixed[c].astype(jnp.float32).reshape(rows, span).astype(jnp.bfloat16)
        at = pl.ds(pl.multiple_of(c * span, span), span)
        update[...] += jnp.dot(every, out_w[at, :], preferred_element_type=jnp.float32)

    @pl.loop(0, pieces)
    def _(c):
        @pl.loop(1, chips - 1)
        def _(turn):
            @pl.loop(0, 2)
            def _(i):
                leftward = lax.rem(i + near, 2)
                q = jnp.where(leftward == 1, turn - (last - me), last - (turn - me))
                goes_right = jnp.logical_and(
                    jnp.logical_and(leftward == 0, me > 0),
                    jnp.logical_and(q > me, q < chips),
                )
                goes_left = jnp.logical_and(
                    jnp.logical_and(leftward == 1, me < last),
                    jnp.logical_and(q >= 0, q < me),
                )

                @pl.when(jnp.logical_or(goes_right, goes_left))
                def _():
                    pass_on(c, q, True)

        finish(c)

        @pl.when(c > 0)
        def _():
            gather(c - 1)

    gather(pieces - 1)
    middle_ref[...] = update[...].astype(middle_ref.dtype)

    @pl.loop(0, pieces)
    def _(c):
        own_pass(c).wait_send()

        @pl.loop(0, chips)
        def _(q):
            for_width(c, lambda size: sib_copy(c, q, size).wait_send())

        @pl.loop(1, chips)
        def _(step):
            q = lax.rem(me + step, chips)
            mix_copy(c, q).wait_send()
            pass_copy(c, q * 2 + core, pass_send.at[c, q]).wait_send()
            for_width(c, lambda size: chain_copy(c, q, size).wait_send())


def mixer(own, gain, weights, output_weight, carried, floor, head_gain, chips, collective_id):
    rows, width = own.shape
    seqs, head_count, key_size, value_size = carried.shape
    blocks = chips * 2
    pieces = 4
    heads = head_count // pieces
    span = heads * key_size
    extent = 4 * span + LANES
    dma = pltpu.SemaphoreType.DMA
    vmem = pl.BlockSpec(memory_space=pltpu.VMEM)
    hbm = pl.BlockSpec(memory_space=pl.ANY)
    lines = jax.ShapeDtypeStruct((pieces, seqs, span), jnp.float32)
    return pl.pallas_call(
        functools.partial(mixer_kernel, chips, pieces),
        out_shape=(jax.ShapeDtypeStruct((rows, width), jnp.bfloat16), lines, lines),
        in_specs=[vmem] * 4 + [hbm] * 6,
        out_specs=(vmem, vmem, vmem),
        scratch_shapes=[
            pltpu.VMEM((pieces, 4, width, span), jnp.bfloat16),
            pltpu.VMEM(output_weight.shape, jnp.bfloat16),
            pltpu.VMEM((pieces, seqs, heads, key_size, value_size), jnp.float32),
            pltpu.VMEM((rows, width), jnp.bfloat16),
            pltpu.VMEM((pieces, blocks, seqs, extent), jnp.bfloat16),
            pltpu.VMEM((pieces, chips, seqs, extent), jnp.bfloat16),
            pltpu.VMEM((pieces, chips, seqs, extent), jnp.bfloat16),
            pltpu.VMEM((pieces, chips + 1, seqs, extent), jnp.bfloat16),
            pltpu.VMEM((seqs, extent), jnp.float32),
            pltpu.VMEM((seqs, LANES), jnp.float32),
            pltpu.VMEM((16, 8 * LANES), jnp.bfloat16),
            pltpu.VMEM((seqs, span), jnp.float32),
            pltpu.VMEM((seqs, span), jnp.float32),
            pltpu.VMEM((pieces, seqs, span), jnp.bfloat16),
            pltpu.VMEM((pieces, blocks, seqs, span), jnp.bfloat16),
            pltpu.VMEM((rows, width), jnp.float32),
            dma((pieces, 4)),
            dma,
            dma((pieces,)),
            dma((pieces, chips)),
            dma((pieces, chips)),
            dma((pieces, chips)),
            dma((pieces, chips + 1)),
            dma((pieces, chips)),
            dma((pieces, chips)),
            dma((pieces, blocks)),
        ],
        compiler_params=pltpu.CompilerParams(
            collective_id=collective_id, has_side_effects=True, vmem_limit_bytes=VMEM_LIMIT
        ),
    )(
        own,
        gain.reshape(blocks, 1, width),
        floor.reshape(pieces, 1, span),
        head_gain.reshape(1, value_size),
        *weights,
        output_weight,
        carried,
    )


def state_kernel(old_ref, forget_ref, value_ref, new_ref):
    rows, heads = old_ref.shape[:2]
    groups, _, span = forget_ref.shape
    pick = picker()
    per = span // LANES
    for h in range(heads):
        group = h // per
        lanes = slice((h % per) * LANES, (h % per + 1) * LANES)
        wide = spread(forget_ref[group, :, lanes], pick)
        for s in range(rows):
            value = value_ref[group, s : s + 1, lanes]
            new_ref[s, h] = value + wide[:, s * LANES : (s + 1) * LANES] * (old_ref[s, h] - value)


def update_state(carried, forget, value):
    rows, heads, keys, values = carried.shape
    pieces, _, span = forget.shape
    batch = 8
    cut = span // keys * (2 if pieces % 2 == 0 else 1)
    groups = cut * keys // span
    cells = rows * heads * keys * values
    lines = pl.BlockSpec((groups, batch, span), lambda i, j: (j, i, 0))
    grid = pl.BlockSpec((batch, cut, keys, values), lambda i, j: (i, j, 0, 0))
    return pl.pallas_call(
        state_kernel,
        grid=(rows // batch, heads // cut),
        out_shape=jax.ShapeDtypeStruct(carried.shape, jnp.float32),
        in_specs=[grid, lines, lines],
        out_specs=grid,
        compiler_params=pltpu.CompilerParams(vmem_limit_bytes=32 * 1024 * 1024),
        cost_estimate=pl.CostEstimate(
            flops=20 * cells, bytes_accessed=8 * cells, transcendentals=0
        ),
    )(carried, forget, value)


def per_device(
    tokens,
    carried_state,
    first_gain,
    first_gate,
    first_up,
    first_down,
    mix_gain,
    query_weight,
    forget_weight,
    input_weight,
    outgate_weight,
    forget_floor,
    head_gain,
    output_weight,
    second_gain,
    second_gate,
    second_up,
    second_down,
):
    chips = lax.axis_size("kv")
    mixer_share = feed_forward(tokens, first_gain, first_gate, first_up, first_down, chips, 0)
    middle, forget, value = mixer(
        mixer_share,
        mix_gain,
        (query_weight, forget_weight, input_weight, outgate_weight),
        output_weight,
        carried_state,
        forget_floor,
        head_gain,
        chips,
        1,
    )
    next_state = update_state(carried_state, forget, value)
    layer_out = feed_forward(middle, second_gain, second_gate, second_up, second_down, chips, 2)
    return (layer_out, next_state)


def solution(mesh):
    in_specs = (
        P("dp", ("kv", "tp")),
        P(("dp", "kv", "tp"), None, None, None),
        P(),
        P(None, ("kv", "tp")),
        P(None, ("kv", "tp")),
        P(("kv", "tp"), None),
        P(),
        P(("kv", "tp"), None),
        P(("kv", "tp"), None),
        P(("kv", "tp"), None),
        P(("kv", "tp"), None),
        P(),
        P(),
        P(None, ("kv", "tp")),
        P(),
        P(None, ("kv", "tp")),
        P(None, ("kv", "tp")),
        P(("kv", "tp"), None),
    )
    out_specs = (P("dp", ("kv", "tp")), P(("dp", "kv", "tp"), None, None, None))
    return jax.shard_map(
        per_device, mesh=mesh, in_specs=in_specs, out_specs=out_specs, check_vma=False
    )
```

```python
import functools

import jax
import jax.numpy as jnp
from jax import lax
from jax.experimental import pallas as pl
from jax.experimental.pallas import tpu as pltpu
from jax.sharding import PartitionSpec as P

epsilon = 1e-06
MESH = pl.DeviceIdType.MESH
VMEM_LIMIT = 63 * 1024 * 1024
LANES = 128
CUT = 4


def remote(src, dst, send_sem, recv_sem, kv, tp):
    return pltpu.make_async_remote_copy(
        src_ref=src,
        dst_ref=dst,
        send_sem=send_sem,
        recv_sem=recv_sem,
        device_id={"kv": kv, "tp": tp},
        device_id_type=MESH,
    )


def greet_all(me, core, chips):
    barrier = pltpu.get_barrier_semaphore()
    pl.semaphore_signal(
        barrier, inc=1, device_id={"kv": me, "tp": 1 - core}, device_id_type=MESH
    )
    for step in range(1, chips):
        pl.semaphore_signal(
            barrier,
            inc=1,
            device_id={"kv": lax.rem(me + step, chips), "tp": core},
            device_id_type=MESH,
        )
    pl.semaphore_wait(barrier, chips)


def greet_chain(me, core, chips):
    barrier = pltpu.get_barrier_semaphore()
    pl.semaphore_signal(
        barrier, inc=1, device_id={"kv": me, "tp": 1 - core}, device_id_type=MESH
    )

    @pl.when(me > 0)
    def _():
        pl.semaphore_signal(
            barrier, inc=1, device_id={"kv": me - 1, "tp": core}, device_id_type=MESH
        )

    @pl.when(me < chips - 1)
    def _():
        pl.semaphore_signal(
            barrier, inc=1, device_id={"kv": me + 1, "tp": core}, device_id_type=MESH
        )

    ends = jnp.where(me > 0, 1, 0) + jnp.where(me < chips - 1, 1, 0)
    pl.semaphore_wait(barrier, 1 + ends)


def block_kernel(
    chips,
    own_hbm,
    gain_hbm,
    gate_hbm,
    up_hbm,
    down_hbm,
    out_ref,
    gate_w,
    up_w,
    down_w,
    cols,
    gain_ref,
    gate_acc,
    up_acc,
    squares,
    hidden,
    held,
    sib_out,
    sib_in,
    chip_out,
    chip_in,
    gate_sem,
    up_sem,
    down_sem,
    local_sem,
    gain_sem,
    fwd_send,
    pass_send,
    recv_sem,
    sib_send,
    sib_recv,
    chip_send,
    chip_recv,
):
    me = lax.axis_index("kv")
    core = lax.axis_index("tp")
    mine = me * 2 + core
    last = chips - 1
    rows, width = own_hbm.shape
    full_width = width * chips * 2
    half = rows // 2
    subs = (0, 1)

    def piece(sub):
        return pl.ds(sub * half, half)

    def gate_copy(j):
        at = pl.ds(pl.multiple_of(j * width, width), width)
        return pltpu.make_async_copy(gate_hbm.at[at, :], gate_w.at[j], gate_sem.at[j])

    def up_copy(j):
        at = pl.ds(pl.multiple_of(j * width, width), width)
        return pltpu.make_async_copy(up_hbm.at[at, :], up_w.at[j], up_sem.at[j])

    def down_copy(j):
        at = pl.ds(pl.multiple_of(j * width, width), width)
        return pltpu.make_async_copy(down_hbm.at[:, at], down_w.at[j], down_sem.at[j])

    own_ref = cols.at[mine]
    local = pltpu.make_async_copy(own_hbm, own_ref, local_sem)
    local.start()
    gains = pltpu.make_async_copy(gain_hbm, gain_ref, gain_sem)
    gains.start()

    def reach(step, side):
        j = me + step * (2 * side - 1)
        fits = jnp.logical_and(j >= 0, j < chips)
        return j, jnp.logical_and(fits, jnp.logical_or(step > 0, side == 0))

    def each_block(body):
        @pl.loop(0, chips)
        def _(step):
            @pl.loop(0, 4)
            def _(i):
                j, valid = reach(step, lax.rem(i, 2))
                other = lax.div(i, 2)

                @pl.when(valid)
                def _():
                    body(j * 2 + lax.rem(core + other, 2))

    def start_in(slot):
        gate_copy(slot).start()
        up_copy(slot).start()

    each_block(start_in)
    greet_chain(me, core, chips)
    local.wait()

    def own_copy(to, tp, sem, sub):
        at = piece(sub)
        return remote(
            own_ref.at[at], cols.at[mine, at], sem, recv_sem.at[mine, sub], to, tp
        )

    def right_copy(sub):
        return own_copy(me + 1, core, fwd_send.at[me, sub], sub)

    def left_copy(sub):
        return own_copy(me - 1, core, fwd_send.at[chips, sub], sub)

    def own_pass(sub):
        return own_copy(me, 1 - core, pass_send.at[me, sub], sub)

    def slot_copy(slot, sub, sem, to, tp):
        at = piece(sub)
        return remote(
            cols.at[slot, at], cols.at[slot, at], sem, recv_sem.at[slot, sub], to, tp
        )

    def fwd_copy(j, sub):
        to = jnp.where(j < me, me + 1, me - 1)
        return slot_copy(j * 2 + core, sub, fwd_send.at[j, sub], to, core)

    def pass_copy(j, sub):
        return slot_copy(j * 2 + core, sub, pass_send.at[j, sub], me, 1 - core)

    def forwards(j):
        return jnp.logical_or(
            jnp.logical_and(j < me, me < last), jnp.logical_and(j > me, me > 0)
        )

    for sub in subs:

        @pl.when(me < last)
        def _():
            right_copy(sub).start()

        @pl.when(me > 0)
        def _():
            left_copy(sub).start()

    for sub in subs:
        own_pass(sub).start()

    def start_down(q):
        down_copy(q * 2 + 1 - core).start()
        down_copy(q * 2 + core).start()

    def far_first(body):
        @pl.loop(0, chips)
        def _(turn):
            @pl.loop(0, 2)
            def _(side):
                q, valid = reach(last - turn, side)

                @pl.when(valid)
                def _():
                    body(q)

    far_first(start_down)

    gate_acc[...] = jnp.zeros_like(gate_acc)
    up_acc[...] = jnp.zeros_like(up_acc)
    squares[...] = jnp.zeros_like(squares)
    gains.wait()

    def take(j):
        block = cols[j].astype(jnp.float32)
        squares[...] += jnp.sum(block * block, axis=1, keepdims=True)
        scaled = (block * gain_ref[j]).astype(jnp.bfloat16)
        gate_copy(j).wait()
        gate_acc[...] += jnp.dot(scaled, gate_w[j], preferred_element_type=jnp.float32)
        up_copy(j).wait()
        up_acc[...] += jnp.dot(scaled, up_w[j], preferred_element_type=jnp.float32)

    @pl.loop(0, chips)
    def _(step):
        @pl.when(step > 0)
        def _():
            for sub in subs:
                for side in (0, 1):
                    j, valid = reach(step, side)

                    @pl.when(valid)
                    def _():
                        pass_copy(j, sub).wait_recv()

                        @pl.when(forwards(j))
                        def _():
                            fwd_copy(j, sub).start()

                        pass_copy(j, sub).start()

        @pl.loop(0, 4)
        def _(i):
            j, valid = reach(step, lax.rem(i, 2))
            other = lax.div(i, 2)
            slot = j * 2 + lax.rem(core + other, 2)

            @pl.when(valid)
            def _():
                @pl.when(other == 1)
                def _():
                    for sub in subs:
                        slot_copy(slot, sub, fwd_send.at[0, 0], me, 1 - core).wait_recv()

                take(slot)

    tile = 32

    @pl.loop(0, rows // tile)
    def _(i):
        at = pl.ds(pl.multiple_of(i * tile, tile), tile)
        row_scale = lax.rsqrt(squares[at, :] / full_width + epsilon)
        gate = row_scale * gate_acc[at, :]
        hidden[at, :] = (gate * jax.nn.sigmoid(gate) * (row_scale * up_acc[at, :])).astype(
            jnp.bfloat16
        )

    def branch(j):
        down_copy(j).wait()
        return 0.5 * jnp.dot(hidden[...], down_w[j], preferred_element_type=jnp.float32)

    def sib_copy(q):
        return remote(
            sib_out.at[q], sib_in.at[q], sib_send.at[q], sib_recv.at[q], me, 1 - core
        )

    def chain_copy(q, sub):
        at = piece(sub)
        to = jnp.where(q > me, me + 1, me - 1)
        slot = jnp.where(q == me - 1, chips, q)
        return remote(
            chip_out.at[q, at],
            chip_in.at[slot, at],
            chip_send.at[q, sub],
            chip_recv.at[slot, sub],
            to,
            core,
        )

    def arrived(slot, sub):
        at = piece(sub)
        remote(
            chip_in.at[slot, at],
            chip_in.at[slot, at],
            chip_send.at[0, sub],
            chip_recv.at[slot, sub],
            me,
            1 - core,
        ).wait_recv()

    def produce(q):
        sib_out[q] = branch(q * 2 + 1 - core).astype(jnp.bfloat16)
        sib_copy(q).start()
        held[q] = branch(q * 2 + core)
        first = jnp.logical_or(
            jnp.logical_and(q > me, me == 0), jnp.logical_and(q < me, me == last)
        )

        @pl.when(first)
        def _():
            sib_copy(q).wait_recv()
            for sub in subs:
                at = piece(sub)
                chip_out[q, at] = (held[q, at] + sib_in[q, at].astype(jnp.float32)).astype(
                    jnp.bfloat16
                )
                chain_copy(q, sub).start()

    far_first(produce)

    near = jnp.where(me <= last - me, 0, 1)

    @pl.loop(1, chips - 1)
    def _(turn):
        for sub in subs:

            @pl.loop(0, 2)
            def _(i):
                leftward = lax.rem(i + near, 2)
                q = jnp.where(leftward == 1, turn - (last - me), last - (turn - me))
                goes_right = jnp.logical_and(
                    jnp.logical_and(leftward == 0, me > 0),
                    jnp.logical_and(q > me, q < chips),
                )
                goes_left = jnp.logical_and(
                    jnp.logical_and(leftward == 1, me < last),
                    jnp.logical_and(q >= 0, q < me),
                )

                @pl.when(jnp.logical_or(goes_right, goes_left))
                def _():
                    if sub == 0:
                        sib_copy(q).wait_recv()
                    arrived(q, sub)
                    at = piece(sub)
                    chip_out[q, at] = (
                        held[q, at]
                        + sib_in[q, at].astype(jnp.float32)
                        + chip_in[q, at].astype(jnp.float32)
                    ).astype(jnp.bfloat16)
                    chain_copy(q, sub).start()

    sib_copy(me).wait_recv()
    for sub in subs:
        at = piece(sub)
        held[me, at] += sib_in[me, at].astype(jnp.float32)

        @pl.when(me > 0)
        def _():
            arrived(me, sub)
            held[me, at] += chip_in[me, at].astype(jnp.float32)

        @pl.when(me < last)
        def _():
            arrived(chips, sub)
            held[me, at] += chip_in[chips, at].astype(jnp.float32)

        out_ref[at] = (held[me, at] + cols[mine, at].astype(jnp.float32)).astype(out_ref.dtype)

    for sub in subs:

        @pl.when(me < last)
        def _():
            right_copy(sub).wait_send()

        @pl.when(me > 0)
        def _():
            left_copy(sub).wait_send()

    @pl.loop(0, chips)
    def _(j):
        sib_copy(j).wait_send()
        for sub in subs:
            pass_copy(j, sub).wait_send()

            @pl.when(forwards(j))
            def _():
                fwd_copy(j, sub).wait_send()

            @pl.when(j != me)
            def _():
                chain_copy(j, sub).wait_send()


def feed_forward(own, gain, gate, up, down, chips, collective_id):
    rows, width = own.shape
    units = gate.shape[1]
    blocks = chips * 2
    dma = pltpu.SemaphoreType.DMA
    half_rounds = (chips, rows, width)
    return pl.pallas_call(
        functools.partial(block_kernel, chips),
        out_shape=jax.ShapeDtypeStruct((rows, width), jnp.bfloat16),
        in_specs=[pl.BlockSpec(memory_space=pl.ANY)] * 5,
        out_specs=pl.BlockSpec(memory_space=pltpu.VMEM),
        scratch_shapes=[
            pltpu.VMEM((blocks, width, units), jnp.bfloat16),
            pltpu.VMEM((blocks, width, units), jnp.bfloat16),
            pltpu.VMEM((blocks, units, width), jnp.bfloat16),
            pltpu.VMEM((blocks, rows, width), jnp.bfloat16),
            pltpu.VMEM((blocks, 1, width), jnp.float32),
            pltpu.VMEM((rows, units), jnp.float32),
            pltpu.VMEM((rows, units), jnp.float32),
            pltpu.VMEM((rows, 1), jnp.float32),
            pltpu.VMEM((rows, units), jnp.bfloat16),
            pltpu.VMEM(half_rounds, jnp.float32),
            pltpu.VMEM(half_rounds, jnp.bfloat16),
            pltpu.VMEM(half_rounds, jnp.bfloat16),
            pltpu.VMEM(half_rounds, jnp.bfloat16),
            pltpu.VMEM((chips + 1, rows, width), jnp.bfloat16),
            dma((blocks,)),
            dma((blocks,)),
            dma((blocks,)),
            dma,
            dma,
            dma((chips + 1, 2)),
            dma((chips, 2)),
            dma((blocks, 2)),
            dma((chips,)),
            dma((chips,)),
            dma((chips, 2)),
            dma((chips + 1, 2)),
        ],
        compiler_params=pltpu.CompilerParams(
            collective_id=collective_id, has_side_effects=True, vmem_limit_bytes=VMEM_LIMIT
        ),
    )(own, gain.reshape(blocks, 1, width), gate, up, down)


def picker():
    row = lax.broadcasted_iota(jnp.int32, (16, 8 * LANES), 0)
    col = lax.broadcasted_iota(jnp.int32, (16, 8 * LANES), 1)
    return (lax.rem(row, 8) == lax.div(col, LANES)).astype(jnp.bfloat16)


def spread(eight, pick):
    high = eight.astype(jnp.bfloat16).astype(jnp.float32)
    both = jnp.concatenate([high, eight - high], axis=0).astype(jnp.bfloat16)
    return lax.dot_general(
        both, pick, (((0,), (0,)), ((), ())), preferred_element_type=jnp.float32
    )


def encode(total):
    lane = lax.broadcasted_iota(jnp.int32, (total.shape[0], LANES), 1)
    high = total.astype(jnp.bfloat16).astype(jnp.float32)
    return jnp.where(lane < LANES // 2, high, total - high)


def decode(pairs):
    return jnp.sum(pairs, axis=1, keepdims=True) * (2.0 / LANES)


def mixer_kernel(
    chips,
    pieces,
    own_hbm,
    gain_hbm,
    floor_hbm,
    head_hbm,
    query_hbm,
    forget_hbm,
    input_hbm,
    outgate_hbm,
    output_hbm,
    state_hbm,
    middle_ref,
    forget_ref,
    value_ref,
    own_ref,
    gain_ref,
    floor_ref,
    head_ref,
    weights,
    out_w,
    state,
    scaled,
    part,
    sib_in,
    chip_out,
    chip_in,
    total,
    scale,
    pick,
    mass,
    readout,
    mix_own,
    mixed,
    update,
    small_sem,
    weight_sem,
    out_sem,
    state_sem,
    sib_send,
    sib_recv,
    chip_send,
    chip_recv,
    mix_send,
    pass_send,
    mix_recv,
):
    me = lax.axis_index("kv")
    core = lax.axis_index("tp")
    mine = me * 2 + core
    last = chips - 1
    rows, width = own_hbm.shape
    full_width = width * chips * 2
    blocks = chips * 2
    seqs = rows // blocks
    span = weights.shape[3]
    heads = state.shape[2]
    main = 4 * span
    projections = (query_hbm, forget_hbm, input_hbm, outgate_hbm)

    def weight_copy(c, p):
        at = pl.ds(pl.multiple_of(c * span, span), span)
        return pltpu.make_async_copy(
            projections[p].at[:, at], weights.at[c, p], weight_sem.at[c, p]
        )

    def state_copy(c):
        return pltpu.make_async_copy(
            state_hbm.at[:, pl.ds(c * heads, heads)], state.at[c], state_sem.at[c]
        )

    out_copy = pltpu.make_async_copy(output_hbm, out_w, out_sem)
    small = (
        (own_hbm, own_ref),
        (gain_hbm.at[mine], gain_ref),
        (floor_hbm, floor_ref),
        (head_hbm, head_ref),
    )
    small = [
        pltpu.make_async_copy(src, dst, small_sem.at[i]) for i, (src, dst) in enumerate(small)
    ]
    for copy in small:
        copy.start()

    @pl.loop(0, pieces)
    def _(c):
        for p in range(4):
            weight_copy(c, p).start()

    @pl.loop(0, pieces)
    def _(c):
        state_copy(c).start()

    out_copy.start()
    pick[...] = picker()
    greet_all(me, core, chips)
    for copy in small:
        copy.wait()
    wide = own_ref[...].astype(jnp.float32)
    scaled[...] = (wide * gain_ref[...]).astype(jnp.bfloat16)
    part[0, :, :, main:] = (
        encode(jnp.sum(wide * wide, axis=1, keepdims=True))
        .reshape(blocks, seqs, LANES)
        .astype(jnp.bfloat16)
    )
    update[...] = wide

    def for_width(c, body):
        @pl.when(c == 0)
        def _():
            body(main + LANES)

        @pl.when(c > 0)
        def _():
            body(main)

    def sib_copy(c, q, size):
        at = pl.ds(0, size)
        return remote(
            part.at[c, q * 2 + 1 - core, :, at],
            sib_in.at[c, q, :, at],
            sib_send.at[c, q],
            sib_recv.at[c, q],
            me,
            1 - core,
        )

    def chain_copy(c, q, size):
        at = pl.ds(0, size)
        to = jnp.where(q > me, me + 1, me - 1)
        slot = jnp.where(q == me - 1, chips, q)
        return remote(
            chip_out.at[c, q, :, at],
            chip_in.at[c, slot, :, at],
            chip_send.at[c, q],
            chip_recv.at[c, slot],
            to,
            core,
        )

    def arrived(c, slot, size):
        at = pl.ds(0, size)
        remote(
            chip_in.at[c, slot, :, at],
            chip_in.at[c, slot, :, at],
            chip_send.at[c, 0],
            chip_recv.at[c, slot],
            me,
            1 - core,
        ).wait_recv()

    def local_sum(c, q, at):
        return part[c, q * 2 + core, :, at].astype(jnp.float32) + sib_in[c, q, :, at].astype(
            jnp.float32
        )

    def pass_on(c, q, upstream):
        def body(size):
            sib_copy(c, q, size).wait_recv()
            if upstream:
                arrived(c, q, size)

            def summed(at):
                here = local_sum(c, q, at)
                if upstream:
                    here = here + chip_in[c, q, :, at].astype(jnp.float32)
                return here

            chip_out[c, q, :, :main] = summed(slice(0, main)).astype(jnp.bfloat16)
            if size > main:
                at = slice(main, main + LANES)
                chip_out[c, q, :, at] = encode(decode(summed(at))).astype(jnp.bfloat16)
            chain_copy(c, q, size).start()

        for_width(c, body)

    @pl.loop(0, pieces)
    def _(c):
        for p in range(4):
            weight_copy(c, p).wait()
            part[c, :, :, p * span : (p + 1) * span] = (
                jnp.dot(scaled[...], weights[c, p], preferred_element_type=jnp.float32)
                .reshape(blocks, seqs, span)
                .astype(jnp.bfloat16)
            )

        @pl.loop(0, chips)
        def _(turn):
            q = jnp.where(me * 2 < chips, last - turn, turn)
            for_width(c, lambda size: sib_copy(c, q, size).start())

        @pl.loop(0, chips - 1)
        def _(turn):
            @pl.when(me == 0)
            def _():
                pass_on(c, last - turn, False)

            @pl.when(me == last)
            def _():
                pass_on(c, turn, False)

    near = jnp.where(me <= last - me, 0, 1)

    def mix_copy(c, to):
        return remote(
            mix_own.at[c],
            mixed.at[c, mine],
            mix_send.at[c, to],
            mix_recv.at[c, mine],
            to,
            core,
        )

    def own_pass(c):
        return remote(
            mix_own.at[c],
            mixed.at[c, mine],
            mix_send.at[c, me],
            mix_recv.at[c, mine],
            me,
            1 - core,
        )

    def pass_copy(c, slot, sem):
        return remote(
            mixed.at[c, slot], mixed.at[c, slot], sem, mix_recv.at[c, slot], me, 1 - core
        )

    def finish(c):
        def gather_total(size):
            sib_copy(c, me, size).wait_recv()
            at = slice(0, size)
            total[:, at] = local_sum(c, me, at)

            @pl.when(me > 0)
            def _():
                arrived(c, me, size)
                total[:, at] += chip_in[c, me, :, at].astype(jnp.float32)

            @pl.when(me < last)
            def _():
                arrived(c, chips, size)
                total[:, at] += chip_in[c, chips, :, at].astype(jnp.float32)

        for_width(c, gather_total)

        @pl.when(c == 0)
        def _():
            squares = decode(total[:, main : main + LANES])
            scale[...] = jnp.broadcast_to(
                lax.rsqrt(squares / full_width + epsilon), scale.shape
            )

        row_scale = scale[:, 0:1]
        query = row_scale * total[:, 0:span]
        query = query * jax.nn.sigmoid(query)
        floor = floor_ref[c]
        forget = floor + (1.0 - floor) * jax.nn.sigmoid(row_scale * total[:, span : 2 * span])
        value = row_scale * total[:, 2 * span : 3 * span]
        forget_ref[c] = forget
        value_ref[c] = value
        mass[...] = query * forget
        rest = query - query * forget
        state_copy(c).wait()

        @pl.loop(0, seqs // 8)
        def _(octet):
            at = pl.ds(pl.multiple_of(octet * 8, 8), 8)
            for h in range(heads):
                lanes = slice(h * LANES, (h + 1) * LANES)
                wide_mass = spread(mass[at, lanes], pick[...])
                lines = []
                for i in range(8):
                    old = state[c, octet * 8 + i, h]
                    lines.append(
                        jnp.sum(
                            old * wide_mass[:, i * LANES : (i + 1) * LANES],
                            axis=0,
                            keepdims=True,
                        )
                    )
                readout[at, lanes] = jnp.concatenate(lines, axis=0)

        gate = row_scale * total[:, 3 * span : 4 * span]
        gate = gate * jax.nn.sigmoid(gate)
        for h in range(heads):
            lanes = slice(h * LANES, (h + 1) * LANES)
            read = readout[:, lanes] + value[:, lanes] * jnp.sum(
                rest[:, lanes], axis=1, keepdims=True
            )
            read = (
                read
                * lax.rsqrt(jnp.mean(read * read, axis=1, keepdims=True) + epsilon)
                * head_ref[...]
                * gate[:, lanes]
            )
            mix_own[c, :, lanes] = read.astype(jnp.bfloat16)

        @pl.loop(1, chips)
        def _(step):
            mix_copy(c, lax.rem(me + step, chips)).start()

        own_pass(c).start()
        mixed[c, mine] = mix_own[c]

    def gather(c):
        @pl.loop(1, chips)
        def _(step):
            q = lax.rem(me + step, chips)
            pass_copy(c, q * 2 + core, mix_send.at[c, 0]).wait_recv()
            pass_copy(c, q * 2 + core, pass_send.at[c, q]).start()

        @pl.loop(0, chips)
        def _(q):
            pass_copy(c, q * 2 + 1 - core, mix_send.at[c, 0]).wait_recv()

        @pl.when(c == 0)
        def _():
            out_copy.wait()

        every = mixed[c].astype(jnp.float32).reshape(rows, span).astype(jnp.bfloat16)
        at = pl.ds(pl.multiple_of(c * span, span), span)
        update[...] += jnp.dot(every, out_w[at, :], preferred_element_type=jnp.float32)

    def relay(c):
        @pl.loop(1, chips - 1)
        def _(turn):
            @pl.loop(0, 2)
            def _(i):
                leftward = lax.rem(i + near, 2)
                q = jnp.where(leftward == 1, turn - (last - me), last - (turn - me))
                goes_right = jnp.logical_and(
                    jnp.logical_and(leftward == 0, me > 0),
                    jnp.logical_and(q > me, q < chips),
                )
                goes_left = jnp.logical_and(
                    jnp.logical_and(leftward == 1, me < last),
                    jnp.logical_and(q >= 0, q < me),
                )

                @pl.when(jnp.logical_or(goes_right, goes_left))
                def _():
                    pass_on(c, q, True)

    relay(0)

    @pl.loop(0, pieces)
    def _(c):
        @pl.when(c < pieces - 1)
        def _():
            relay(c + 1)

        finish(c)

        @pl.when(c > 0)
        def _():
            gather(c - 1)

    gather(pieces - 1)
    middle_ref[...] = update[...].astype(middle_ref.dtype)

    @pl.loop(0, pieces)
    def _(c):
        own_pass(c).wait_send()

        @pl.loop(0, chips)
        def _(q):
            for_width(c, lambda size: sib_copy(c, q, size).wait_send())

        @pl.loop(1, chips)
        def _(step):
            q = lax.rem(me + step, chips)
            mix_copy(c, q).wait_send()
            pass_copy(c, q * 2 + core, pass_send.at[c, q]).wait_send()
            for_width(c, lambda size: chain_copy(c, q, size).wait_send())


def mixer(own, gain, weights, output_weight, carried, floor, head_gain, chips, collective_id):
    rows, width = own.shape
    seqs, head_count, key_size, value_size = carried.shape
    blocks = chips * 2
    pieces = 2
    heads = head_count // pieces
    span = heads * key_size
    extent = 4 * span + LANES
    dma = pltpu.SemaphoreType.DMA
    vmem = pl.BlockSpec(memory_space=pltpu.VMEM)
    hbm = pl.BlockSpec(memory_space=pl.ANY)
    lines = jax.ShapeDtypeStruct((pieces, seqs, span), jnp.float32)
    return pl.pallas_call(
        functools.partial(mixer_kernel, chips, pieces),
        out_shape=(jax.ShapeDtypeStruct((rows, width), jnp.bfloat16), lines, lines),
        in_specs=[hbm] * 10,
        out_specs=(vmem, vmem, vmem),
        scratch_shapes=[
            pltpu.VMEM((rows, width), jnp.bfloat16),
            pltpu.VMEM((1, width), jnp.float32),
            pltpu.VMEM((pieces, 1, span), jnp.float32),
            pltpu.VMEM((1, value_size), jnp.float32),
            pltpu.VMEM((pieces, 4, width, span), jnp.bfloat16),
            pltpu.VMEM(output_weight.shape, jnp.bfloat16),
            pltpu.VMEM((pieces, seqs, heads, key_size, value_size), jnp.float32),
            pltpu.VMEM((rows, width), jnp.bfloat16),
            pltpu.VMEM((pieces, blocks, seqs, extent), jnp.bfloat16),
            pltpu.VMEM((pieces, chips, seqs, extent), jnp.bfloat16),
            pltpu.VMEM((pieces, chips, seqs, extent), jnp.bfloat16),
            pltpu.VMEM((pieces, chips + 1, seqs, extent), jnp.bfloat16),
            pltpu.VMEM((seqs, extent), jnp.float32),
            pltpu.VMEM((seqs, LANES), jnp.float32),
            pltpu.VMEM((16, 8 * LANES), jnp.bfloat16),
            pltpu.VMEM((seqs, span), jnp.float32),
            pltpu.VMEM((seqs, span), jnp.float32),
            pltpu.VMEM((pieces, seqs, span), jnp.bfloat16),
            pltpu.VMEM((pieces, blocks, seqs, span), jnp.bfloat16),
            pltpu.VMEM((rows, width), jnp.float32),
            dma((4,)),
            dma((pieces, 4)),
            dma,
            dma((pieces,)),
            dma((pieces, chips)),
            dma((pieces, chips)),
            dma((pieces, chips)),
            dma((pieces, chips + 1)),
            dma((pieces, chips)),
            dma((pieces, chips)),
            dma((pieces, blocks)),
        ],
        compiler_params=pltpu.CompilerParams(
            collective_id=collective_id, has_side_effects=True, vmem_limit_bytes=VMEM_LIMIT
        ),
    )(
        own,
        gain.reshape(blocks, 1, width),
        floor.reshape(pieces, 1, span),
        head_gain.reshape(1, value_size),
        *weights,
        output_weight,
        carried,
    )


def state_kernel(old_ref, forget_ref, value_ref, new_ref):
    rows, heads = old_ref.shape[:2]
    pick = picker()
    for h in range(heads):
        lanes = slice(h * LANES, (h + 1) * LANES)
        wide = spread(forget_ref[0, :, lanes], pick)
        for s in range(rows):
            value = value_ref[0, s : s + 1, lanes]
            new_ref[s, h] = value + wide[:, s * LANES : (s + 1) * LANES] * (old_ref[s, h] - value)


def update_state(carried, forget, value):
    rows, heads, keys, values = carried.shape
    pieces, _, span = forget.shape
    batch = 8
    cut = min(CUT, span // keys)
    inner = span // keys // cut
    cells = rows * heads * keys * values
    lines = pl.BlockSpec((1, batch, cut * keys), lambda i, j: (j // inner, i, j % inner))
    grid = pl.BlockSpec((batch, cut, keys, values), lambda i, j: (i, j, 0, 0))
    return pl.pallas_call(
        state_kernel,
        grid=(rows // batch, heads // cut),
        out_shape=jax.ShapeDtypeStruct(carried.shape, jnp.float32),
        in_specs=[grid, lines, lines],
        out_specs=grid,
        compiler_params=pltpu.CompilerParams(vmem_limit_bytes=32 * 1024 * 1024),
        cost_estimate=pl.CostEstimate(
            flops=20 * cells, bytes_accessed=8 * cells, transcendentals=0
        ),
    )(carried, forget, value)


def per_device(
    tokens,
    carried_state,
    first_gain,
    first_gate,
    first_up,
    first_down,
    mix_gain,
    query_weight,
    forget_weight,
    input_weight,
    outgate_weight,
    forget_floor,
    head_gain,
    output_weight,
    second_gain,
    second_gate,
    second_up,
    second_down,
):
    chips = lax.axis_size("kv")
    mixer_share = feed_forward(tokens, first_gain, first_gate, first_up, first_down, chips, 0)
    middle, forget, value = mixer(
        mixer_share,
        mix_gain,
        (query_weight, forget_weight, input_weight, outgate_weight),
        output_weight,
        carried_state,
        forget_floor,
        head_gain,
        chips,
        1,
    )
    next_state = update_state(carried_state, forget, value)
    layer_out = feed_forward(middle, second_gain, second_gate, second_up, second_down, chips, 2)
    return (layer_out, next_state)


def solution(mesh):
    in_specs = (
        P("dp", ("kv", "tp")),
        P(("dp", "kv", "tp"), None, None, None),
        P(),
        P(None, ("kv", "tp")),
        P(None, ("kv", "tp")),
        P(("kv", "tp"), None),
        P(),
        P(("kv", "tp"), None),
        P(("kv", "tp"), None),
        P(("kv", "tp"), None),
        P(("kv", "tp"), None),
        P(),
        P(),
        P(None, ("kv", "tp")),
        P(),
        P(None, ("kv", "tp")),
        P(None, ("kv", "tp")),
        P(("kv", "tp"), None),
    )
    out_specs = (P("dp", ("kv", "tp")), P(("dp", "kv", "tp"), None, None, None))
    return jax.shard_map(
        per_device, mesh=mesh, in_specs=in_specs, out_specs=out_specs, check_vma=False
    )
```

```python
import functools

import jax
import jax.numpy as jnp
from jax import lax
from jax.experimental import pallas as pl
from jax.experimental.pallas import tpu as pltpu
from jax.sharding import PartitionSpec as P

epsilon = 1e-06
MESH = pl.DeviceIdType.MESH
VMEM_LIMIT = 63 * 1024 * 1024
MIXER_LIMIT = 29 * 1024 * 1024
LANES = 128


def remote(src, dst, send_sem, recv_sem, kv, tp):
    return pltpu.make_async_remote_copy(
        src_ref=src,
        dst_ref=dst,
        send_sem=send_sem,
        recv_sem=recv_sem,
        device_id={"kv": kv, "tp": tp},
        device_id_type=MESH,
    )


def greet_all(me, core, chips):
    barrier = pltpu.get_barrier_semaphore()
    pl.semaphore_signal(
        barrier, inc=1, device_id={"kv": me, "tp": 1 - core}, device_id_type=MESH
    )
    for step in range(1, chips):
        pl.semaphore_signal(
            barrier,
            inc=1,
            device_id={"kv": lax.rem(me + step, chips), "tp": core},
            device_id_type=MESH,
        )
    pl.semaphore_wait(barrier, chips)


def greet_chain(me, core, chips):
    barrier = pltpu.get_barrier_semaphore()
    pl.semaphore_signal(
        barrier, inc=1, device_id={"kv": me, "tp": 1 - core}, device_id_type=MESH
    )

    @pl.when(me > 0)
    def _():
        pl.semaphore_signal(
            barrier, inc=1, device_id={"kv": me - 1, "tp": core}, device_id_type=MESH
        )

    @pl.when(me < chips - 1)
    def _():
        pl.semaphore_signal(
            barrier, inc=1, device_id={"kv": me + 1, "tp": core}, device_id_type=MESH
        )

    ends = jnp.where(me > 0, 1, 0) + jnp.where(me < chips - 1, 1, 0)
    pl.semaphore_wait(barrier, 1 + ends)


def block_kernel(
    chips,
    own_hbm,
    gain_hbm,
    gate_hbm,
    up_hbm,
    down_hbm,
    out_ref,
    gate_w,
    up_w,
    down_w,
    cols,
    gain_ref,
    gate_acc,
    up_acc,
    squares,
    hidden,
    held,
    sib_out,
    sib_in,
    chip_out,
    chip_in,
    gate_sem,
    up_sem,
    down_sem,
    local_sem,
    gain_sem,
    fwd_send,
    pass_send,
    recv_sem,
    sib_send,
    sib_recv,
    chip_send,
    chip_recv,
):
    me = lax.axis_index("kv")
    core = lax.axis_index("tp")
    mine = me * 2 + core
    last = chips - 1
    rows, width = own_hbm.shape
    full_width = width * chips * 2
    half = rows // 2
    subs = (0, 1)

    def piece(sub):
        return pl.ds(sub * half, half)

    def gate_copy(j):
        at = pl.ds(pl.multiple_of(j * width, width), width)
        return pltpu.make_async_copy(gate_hbm.at[at, :], gate_w.at[j], gate_sem.at[j])

    def up_copy(j):
        at = pl.ds(pl.multiple_of(j * width, width), width)
        return pltpu.make_async_copy(up_hbm.at[at, :], up_w.at[j], up_sem.at[j])

    def down_copy(j):
        at = pl.ds(pl.multiple_of(j * width, width), width)
        return pltpu.make_async_copy(down_hbm.at[:, at], down_w.at[j], down_sem.at[j])

    own_ref = cols.at[mine]
    local = pltpu.make_async_copy(own_hbm, own_ref, local_sem)
    local.start()
    gains = pltpu.make_async_copy(gain_hbm, gain_ref, gain_sem)
    gains.start()

    def reach(step, side):
        j = me + step * (2 * side - 1)
        fits = jnp.logical_and(j >= 0, j < chips)
        return j, jnp.logical_and(fits, jnp.logical_or(step > 0, side == 0))

    def each_block(body):
        @pl.loop(0, chips)
        def _(step):
            @pl.loop(0, 4)
            def _(i):
                j, valid = reach(step, lax.rem(i, 2))
                other = lax.div(i, 2)

                @pl.when(valid)
                def _():
                    body(j * 2 + lax.rem(core + other, 2))

    def start_in(slot):
        gate_copy(slot).start()
        up_copy(slot).start()

    each_block(start_in)
    greet_chain(me, core, chips)
    local.wait()

    def own_copy(to, tp, sem, sub):
        at = piece(sub)
        return remote(
            own_ref.at[at], cols.at[mine, at], sem, recv_sem.at[mine, sub], to, tp
        )

    def right_copy(sub):
        return own_copy(me + 1, core, fwd_send.at[me, sub], sub)

    def left_copy(sub):
        return own_copy(me - 1, core, fwd_send.at[chips, sub], sub)

    def own_pass(sub):
        return own_copy(me, 1 - core, pass_send.at[me, sub], sub)

    def slot_copy(slot, sub, sem, to, tp):
        at = piece(sub)
        return remote(
            cols.at[slot, at], cols.at[slot, at], sem, recv_sem.at[slot, sub], to, tp
        )

    def fwd_copy(j, sub):
        to = jnp.where(j < me, me + 1, me - 1)
        return slot_copy(j * 2 + core, sub, fwd_send.at[j, sub], to, core)

    def pass_copy(j, sub):
        return slot_copy(j * 2 + core, sub, pass_send.at[j, sub], me, 1 - core)

    def forwards(j):
        return jnp.logical_or(
            jnp.logical_and(j < me, me < last), jnp.logical_and(j > me, me > 0)
        )

    for sub in subs:

        @pl.when(me < last)
        def _():
            right_copy(sub).start()

        @pl.when(me > 0)
        def _():
            left_copy(sub).start()

    for sub in subs:
        own_pass(sub).start()

    def start_down(q):
        down_copy(q * 2 + 1 - core).start()
        down_copy(q * 2 + core).start()

    def far_first(body):
        @pl.loop(0, chips)
        def _(turn):
            @pl.loop(0, 2)
            def _(side):
                q, valid = reach(last - turn, side)

                @pl.when(valid)
                def _():
                    body(q)

    far_first(start_down)

    gate_acc[...] = jnp.zeros_like(gate_acc)
    up_acc[...] = jnp.zeros_like(up_acc)
    squares[...] = jnp.zeros_like(squares)
    gains.wait()

    def take(j):
        block = cols[j].astype(jnp.float32)
        squares[...] += jnp.sum(block * block, axis=1, keepdims=True)
        scaled = (block * gain_ref[j]).astype(jnp.bfloat16)
        gate_copy(j).wait()
        gate_acc[...] += jnp.dot(scaled, gate_w[j], preferred_element_type=jnp.float32)
        up_copy(j).wait()
        up_acc[...] += jnp.dot(scaled, up_w[j], preferred_element_type=jnp.float32)

    @pl.loop(0, chips)
    def _(step):
        @pl.when(step > 0)
        def _():
            for sub in subs:
                for side in (0, 1):
                    j, valid = reach(step, side)

                    @pl.when(valid)
                    def _():
                        pass_copy(j, sub).wait_recv()

                        @pl.when(forwards(j))
                        def _():
                            fwd_copy(j, sub).start()

                        pass_copy(j, sub).start()

        @pl.loop(0, 4)
        def _(i):
            j, valid = reach(step, lax.rem(i, 2))
            other = lax.div(i, 2)
            slot = j * 2 + lax.rem(core + other, 2)

            @pl.when(valid)
            def _():
                @pl.when(other == 1)
                def _():
                    for sub in subs:
                        slot_copy(slot, sub, fwd_send.at[0, 0], me, 1 - core).wait_recv()

                take(slot)

    tile = 32

    @pl.loop(0, rows // tile)
    def _(i):
        at = pl.ds(pl.multiple_of(i * tile, tile), tile)
        row_scale = lax.rsqrt(squares[at, :] / full_width + epsilon)
        gate = row_scale * gate_acc[at, :]
        hidden[at, :] = (gate * jax.nn.sigmoid(gate) * (row_scale * up_acc[at, :])).astype(
            jnp.bfloat16
        )

    def branch(j):
        down_copy(j).wait()
        return 0.5 * jnp.dot(hidden[...], down_w[j], preferred_element_type=jnp.float32)

    def sib_copy(q):
        return remote(
            sib_out.at[q], sib_in.at[q], sib_send.at[q], sib_recv.at[q], me, 1 - core
        )

    def chain_copy(q, sub):
        at = piece(sub)
        to = jnp.where(q > me, me + 1, me - 1)
        slot = jnp.where(q == me - 1, chips, q)
        return remote(
            chip_out.at[q, at],
            chip_in.at[slot, at],
            chip_send.at[q, sub],
            chip_recv.at[slot, sub],
            to,
            core,
        )

    def arrived(slot, sub):
        at = piece(sub)
        remote(
            chip_in.at[slot, at],
            chip_in.at[slot, at],
            chip_send.at[0, sub],
            chip_recv.at[slot, sub],
            me,
            1 - core,
        ).wait_recv()

    def produce(q):
        sib_out[q] = branch(q * 2 + 1 - core).astype(jnp.bfloat16)
        sib_copy(q).start()
        held[q] = branch(q * 2 + core)
        first = jnp.logical_or(
            jnp.logical_and(q > me, me == 0), jnp.logical_and(q < me, me == last)
        )

        @pl.when(first)
        def _():
            sib_copy(q).wait_recv()
            for sub in subs:
                at = piece(sub)
                chip_out[q, at] = (held[q, at] + sib_in[q, at].astype(jnp.float32)).astype(
                    jnp.bfloat16
                )
                chain_copy(q, sub).start()

    far_first(produce)

    near = jnp.where(me <= last - me, 0, 1)

    @pl.loop(1, chips - 1)
    def _(turn):
        for sub in subs:

            @pl.loop(0, 2)
            def _(i):
                leftward = lax.rem(i + near, 2)
                q = jnp.where(leftward == 1, turn - (last - me), last - (turn - me))
                goes_right = jnp.logical_and(
                    jnp.logical_and(leftward == 0, me > 0),
                    jnp.logical_and(q > me, q < chips),
                )
                goes_left = jnp.logical_and(
                    jnp.logical_and(leftward == 1, me < last),
                    jnp.logical_and(q >= 0, q < me),
                )

                @pl.when(jnp.logical_or(goes_right, goes_left))
                def _():
                    if sub == 0:
                        sib_copy(q).wait_recv()
                    arrived(q, sub)
                    at = piece(sub)
                    chip_out[q, at] = (
                        held[q, at]
                        + sib_in[q, at].astype(jnp.float32)
                        + chip_in[q, at].astype(jnp.float32)
                    ).astype(jnp.bfloat16)
                    chain_copy(q, sub).start()

    sib_copy(me).wait_recv()
    for sub in subs:
        at = piece(sub)
        held[me, at] += sib_in[me, at].astype(jnp.float32)

        @pl.when(me > 0)
        def _():
            arrived(me, sub)
            held[me, at] += chip_in[me, at].astype(jnp.float32)

        @pl.when(me < last)
        def _():
            arrived(chips, sub)
            held[me, at] += chip_in[chips, at].astype(jnp.float32)

        out_ref[at] = (held[me, at] + cols[mine, at].astype(jnp.float32)).astype(out_ref.dtype)

    for sub in subs:

        @pl.when(me < last)
        def _():
            right_copy(sub).wait_send()

        @pl.when(me > 0)
        def _():
            left_copy(sub).wait_send()

    @pl.loop(0, chips)
    def _(j):
        sib_copy(j).wait_send()
        for sub in subs:
            pass_copy(j, sub).wait_send()

            @pl.when(forwards(j))
            def _():
                fwd_copy(j, sub).wait_send()

            @pl.when(j != me)
            def _():
                chain_copy(j, sub).wait_send()


def feed_forward(own, gain, gate, up, down, chips, collective_id):
    rows, width = own.shape
    units = gate.shape[1]
    blocks = chips * 2
    dma = pltpu.SemaphoreType.DMA
    half_rounds = (chips, rows, width)
    return pl.pallas_call(
        functools.partial(block_kernel, chips),
        out_shape=jax.ShapeDtypeStruct((rows, width), jnp.bfloat16),
        in_specs=[pl.BlockSpec(memory_space=pl.ANY)] * 5,
        out_specs=pl.BlockSpec(memory_space=pltpu.VMEM),
        scratch_shapes=[
            pltpu.VMEM((blocks, width, units), jnp.bfloat16),
            pltpu.VMEM((blocks, width, units), jnp.bfloat16),
            pltpu.VMEM((blocks, units, width), jnp.bfloat16),
            pltpu.VMEM((blocks, rows, width), jnp.bfloat16),
            pltpu.VMEM((blocks, 1, width), jnp.float32),
            pltpu.VMEM((rows, units), jnp.float32),
            pltpu.VMEM((rows, units), jnp.float32),
            pltpu.VMEM((rows, 1), jnp.float32),
            pltpu.VMEM((rows, units), jnp.bfloat16),
            pltpu.VMEM(half_rounds, jnp.float32),
            pltpu.VMEM(half_rounds, jnp.bfloat16),
            pltpu.VMEM(half_rounds, jnp.bfloat16),
            pltpu.VMEM(half_rounds, jnp.bfloat16),
            pltpu.VMEM((chips + 1, rows, width), jnp.bfloat16),
            dma((blocks,)),
            dma((blocks,)),
            dma((blocks,)),
            dma,
            dma,
            dma((chips + 1, 2)),
            dma((chips, 2)),
            dma((blocks, 2)),
            dma((chips,)),
            dma((chips,)),
            dma((chips, 2)),
            dma((chips + 1, 2)),
        ],
        compiler_params=pltpu.CompilerParams(
            collective_id=collective_id, has_side_effects=True, vmem_limit_bytes=VMEM_LIMIT
        ),
    )(own, gain.reshape(blocks, 1, width), gate, up, down)


def picker():
    row = lax.broadcasted_iota(jnp.int32, (16, 8 * LANES), 0)
    col = lax.broadcasted_iota(jnp.int32, (16, 8 * LANES), 1)
    return (lax.rem(row, 8) == lax.div(col, LANES)).astype(jnp.bfloat16)


def spread(eight, pick):
    high = eight.astype(jnp.bfloat16).astype(jnp.float32)
    both = jnp.concatenate([high, eight - high], axis=0).astype(jnp.bfloat16)
    return lax.dot_general(
        both, pick, (((0,), (0,)), ((), ())), preferred_element_type=jnp.float32
    )


def encode(total):
    lane = lax.broadcasted_iota(jnp.int32, (total.shape[0], LANES), 1)
    high = total.astype(jnp.bfloat16).astype(jnp.float32)
    return jnp.where(lane < LANES // 2, high, total - high)


def decode(pairs):
    return jnp.sum(pairs, axis=1, keepdims=True) * (2.0 / LANES)


def mixer_kernel(
    chips,
    pieces,
    own_hbm,
    gain_hbm,
    floor_hbm,
    head_hbm,
    query_hbm,
    forget_hbm,
    input_hbm,
    outgate_hbm,
    output_hbm,
    state_hbm,
    middle_ref,
    state,
    own_ref,
    gain_ref,
    floor_ref,
    head_ref,
    weights,
    out_w,
    forget_ref,
    value_ref,
    scaled,
    part,
    sib_in,
    chip_out,
    chip_in,
    total,
    scale,
    pick,
    mass,
    readout,
    mix_own,
    mixed,
    update,
    small_sem,
    weight_sem,
    out_sem,
    state_sem,
    sib_send,
    sib_recv,
    chip_send,
    chip_recv,
    mix_send,
    pass_send,
    mix_recv,
):
    me = lax.axis_index("kv")
    core = lax.axis_index("tp")
    mine = me * 2 + core
    last = chips - 1
    rows, width = own_hbm.shape
    full_width = width * chips * 2
    blocks = chips * 2
    seqs = rows // blocks
    span = weights.shape[3]
    heads = state.shape[1] // pieces
    main = 4 * span
    projections = (query_hbm, forget_hbm, input_hbm, outgate_hbm)

    def weight_copy(c, p):
        at = pl.ds(pl.multiple_of(c * span, span), span)
        return pltpu.make_async_copy(
            projections[p].at[:, at], weights.at[c, p], weight_sem.at[c, p]
        )

    def state_copy(c):
        return pltpu.make_async_copy(
            state_hbm.at[:, pl.ds(c * heads, heads)],
            state.at[:, pl.ds(c * heads, heads)],
            state_sem.at[c],
        )

    out_copy = pltpu.make_async_copy(output_hbm, out_w, out_sem)
    small = (
        (own_hbm, own_ref),
        (gain_hbm.at[mine], gain_ref),
        (floor_hbm, floor_ref),
        (head_hbm, head_ref),
    )
    small = [
        pltpu.make_async_copy(src, dst, small_sem.at[i]) for i, (src, dst) in enumerate(small)
    ]
    for copy in small:
        copy.start()

    @pl.loop(0, pieces)
    def _(c):
        for p in range(4):
            weight_copy(c, p).start()

    @pl.loop(0, pieces)
    def _(c):
        state_copy(c).start()

    out_copy.start()
    pick[...] = picker()
    greet_all(me, core, chips)
    for copy in small:
        copy.wait()
    wide = own_ref[...].astype(jnp.float32)
    scaled[...] = (wide * gain_ref[...]).astype(jnp.bfloat16)
    part[0, :, :, main:] = (
        encode(jnp.sum(wide * wide, axis=1, keepdims=True))
        .reshape(blocks, seqs, LANES)
        .astype(jnp.bfloat16)
    )
    update[...] = wide

    def for_width(c, body):
        @pl.when(c == 0)
        def _():
            body(main + LANES)

        @pl.when(c > 0)
        def _():
            body(main)

    def sib_copy(c, q, size):
        at = pl.ds(0, size)
        return remote(
            part.at[c, q * 2 + 1 - core, :, at],
            sib_in.at[c, q, :, at],
            sib_send.at[c, q],
            sib_recv.at[c, q],
            me,
            1 - core,
        )

    def chain_copy(c, q, size):
        at = pl.ds(0, size)
        to = jnp.where(q > me, me + 1, me - 1)
        slot = jnp.where(q == me - 1, chips, q)
        return remote(
            chip_out.at[c, q, :, at],
            chip_in.at[c, slot, :, at],
            chip_send.at[c, q],
            chip_recv.at[c, slot],
            to,
            core,
        )

    def arrived(c, slot, size):
        at = pl.ds(0, size)
        remote(
            chip_in.at[c, slot, :, at],
            chip_in.at[c, slot, :, at],
            chip_send.at[c, 0],
            chip_recv.at[c, slot],
            me,
            1 - core,
        ).wait_recv()

    def local_sum(c, q, at):
        return part[c, q * 2 + core, :, at].astype(jnp.float32) + sib_in[c, q, :, at].astype(
            jnp.float32
        )

    def pass_on(c, q, upstream):
        def body(size):
            sib_copy(c, q, size).wait_recv()
            if upstream:
                arrived(c, q, size)

            def summed(at):
                here = local_sum(c, q, at)
                if upstream:
                    here = here + chip_in[c, q, :, at].astype(jnp.float32)
                return here

            chip_out[c, q, :, :main] = summed(slice(0, main)).astype(jnp.bfloat16)
            if size > main:
                at = slice(main, main + LANES)
                chip_out[c, q, :, at] = encode(decode(summed(at))).astype(jnp.bfloat16)
            chain_copy(c, q, size).start()

        for_width(c, body)

    @pl.loop(0, pieces)
    def _(c):
        for p in range(4):
            weight_copy(c, p).wait()
            part[c, :, :, p * span : (p + 1) * span] = (
                jnp.dot(scaled[...], weights[c, p], preferred_element_type=jnp.float32)
                .reshape(blocks, seqs, span)
                .astype(jnp.bfloat16)
            )

        @pl.loop(0, chips)
        def _(turn):
            q = jnp.where(me * 2 < chips, last - turn, turn)
            for_width(c, lambda size: sib_copy(c, q, size).start())

        @pl.loop(0, chips - 1)
        def _(turn):
            @pl.when(me == 0)
            def _():
                pass_on(c, last - turn, False)

            @pl.when(me == last)
            def _():
                pass_on(c, turn, False)

    near = jnp.where(me <= last - me, 0, 1)

    def mix_copy(c, to):
        return remote(
            mix_own.at[c],
            mixed.at[c, mine],
            mix_send.at[c, to],
            mix_recv.at[c, mine],
            to,
            core,
        )

    def own_pass(c):
        return remote(
            mix_own.at[c],
            mixed.at[c, mine],
            mix_send.at[c, me],
            mix_recv.at[c, mine],
            me,
            1 - core,
        )

    def pass_copy(c, slot, sem):
        return remote(
            mixed.at[c, slot], mixed.at[c, slot], sem, mix_recv.at[c, slot], me, 1 - core
        )

    def finish(c):
        def gather_total(size):
            sib_copy(c, me, size).wait_recv()
            at = slice(0, size)
            total[:, at] = local_sum(c, me, at)

            @pl.when(me > 0)
            def _():
                arrived(c, me, size)
                total[:, at] += chip_in[c, me, :, at].astype(jnp.float32)

            @pl.when(me < last)
            def _():
                arrived(c, chips, size)
                total[:, at] += chip_in[c, chips, :, at].astype(jnp.float32)

        for_width(c, gather_total)

        @pl.when(c == 0)
        def _():
            squares = decode(total[:, main : main + LANES])
            scale[...] = jnp.broadcast_to(
                lax.rsqrt(squares / full_width + epsilon), scale.shape
            )

        row_scale = scale[:, 0:1]
        query = row_scale * total[:, 0:span]
        query = query * jax.nn.sigmoid(query)
        floor = floor_ref[c]
        forget = floor + (1.0 - floor) * jax.nn.sigmoid(row_scale * total[:, span : 2 * span])
        value = row_scale * total[:, 2 * span : 3 * span]
        forget_ref[c] = forget
        value_ref[c] = value
        mass[...] = query * forget
        rest = query - query * forget
        state_copy(c).wait()

        @pl.loop(0, seqs // 8)
        def _(octet):
            at = pl.ds(pl.multiple_of(octet * 8, 8), 8)
            for h in range(heads):
                lanes = slice(h * LANES, (h + 1) * LANES)
                wide_mass = spread(mass[at, lanes], pick[...])
                lines = []
                for i in range(8):
                    old = state[octet * 8 + i, c * heads + h]
                    lines.append(
                        jnp.sum(
                            old * wide_mass[:, i * LANES : (i + 1) * LANES],
                            axis=0,
                            keepdims=True,
                        )
                    )
                readout[at, lanes] = jnp.concatenate(lines, axis=0)

        gate = row_scale * total[:, 3 * span : 4 * span]
        gate = gate * jax.nn.sigmoid(gate)
        for h in range(heads):
            lanes = slice(h * LANES, (h + 1) * LANES)
            read = readout[:, lanes] + value[:, lanes] * jnp.sum(
                rest[:, lanes], axis=1, keepdims=True
            )
            read = (
                read
                * lax.rsqrt(jnp.mean(read * read, axis=1, keepdims=True) + epsilon)
                * head_ref[...]
                * gate[:, lanes]
            )
            mix_own[c, :, lanes] = read.astype(jnp.bfloat16)

        @pl.loop(1, chips)
        def _(step):
            mix_copy(c, lax.rem(me + step, chips)).start()

        own_pass(c).start()
        mixed[c, mine] = mix_own[c]

        @pl.loop(0, seqs // 8)
        def _(octet):
            at = pl.ds(pl.multiple_of(octet * 8, 8), 8)
            for h in range(heads):
                lanes = slice(h * LANES, (h + 1) * LANES)
                wide_keep = spread(forget_ref[c, at, lanes], pick[...])
                values = value_ref[c, at, lanes]
                for i in range(8):
                    line = values[i : i + 1]
                    keep = wide_keep[:, i * LANES : (i + 1) * LANES]
                    old = state[octet * 8 + i, c * heads + h]
                    state[octet * 8 + i, c * heads + h] = line + keep * (old - line)

    def gather(c):
        @pl.loop(1, chips)
        def _(step):
            q = lax.rem(me + step, chips)
            pass_copy(c, q * 2 + core, mix_send.at[c, 0]).wait_recv()
            pass_copy(c, q * 2 + core, pass_send.at[c, q]).start()

        @pl.loop(0, chips)
        def _(q):
            pass_copy(c, q * 2 + 1 - core, mix_send.at[c, 0]).wait_recv()

        @pl.when(c == 0)
        def _():
            out_copy.wait()

        every = mixed[c].astype(jnp.float32).reshape(rows, span).astype(jnp.bfloat16)
        at = pl.ds(pl.multiple_of(c * span, span), span)
        update[...] += jnp.dot(every, out_w[at, :], preferred_element_type=jnp.float32)

    def relay(c):
        @pl.loop(1, chips - 1)
        def _(turn):
            @pl.loop(0, 2)
            def _(i):
                leftward = lax.rem(i + near, 2)
                q = jnp.where(leftward == 1, turn - (last - me), last - (turn - me))
                goes_right = jnp.logical_and(
                    jnp.logical_and(leftward == 0, me > 0),
                    jnp.logical_and(q > me, q < chips),
                )
                goes_left = jnp.logical_and(
                    jnp.logical_and(leftward == 1, me < last),
                    jnp.logical_and(q >= 0, q < me),
                )

                @pl.when(jnp.logical_or(goes_right, goes_left))
                def _():
                    pass_on(c, q, True)

    relay(0)

    @pl.loop(0, pieces)
    def _(c):
        @pl.when(c < pieces - 1)
        def _():
            relay(c + 1)

        finish(c)

        @pl.when(c > 0)
        def _():
            gather(c - 1)

    gather(pieces - 1)
    middle_ref[...] = update[...].astype(middle_ref.dtype)

    @pl.loop(0, pieces)
    def _(c):
        own_pass(c).wait_send()

        @pl.loop(0, chips)
        def _(q):
            for_width(c, lambda size: sib_copy(c, q, size).wait_send())

        @pl.loop(1, chips)
        def _(step):
            q = lax.rem(me + step, chips)
            mix_copy(c, q).wait_send()
            pass_copy(c, q * 2 + core, pass_send.at[c, q]).wait_send()
            for_width(c, lambda size: chain_copy(c, q, size).wait_send())


def mixer(own, gain, weights, output_weight, carried, floor, head_gain, chips, collective_id):
    rows, width = own.shape
    seqs, head_count, key_size, value_size = carried.shape
    blocks = chips * 2
    pieces = 2
    heads = head_count // pieces
    span = heads * key_size
    extent = 4 * span + LANES
    dma = pltpu.SemaphoreType.DMA
    vmem = pl.BlockSpec(memory_space=pltpu.VMEM)
    hbm = pl.BlockSpec(memory_space=pl.ANY)
    return pl.pallas_call(
        functools.partial(mixer_kernel, chips, pieces),
        out_shape=(
            jax.ShapeDtypeStruct((rows, width), jnp.bfloat16),
            pltpu.VMEM(carried.shape, jnp.float32),
        ),
        in_specs=[hbm] * 10,
        out_specs=(vmem, vmem),
        scratch_shapes=[
            pltpu.VMEM((rows, width), jnp.bfloat16),
            pltpu.VMEM((1, width), jnp.float32),
            pltpu.VMEM((pieces, 1, span), jnp.float32),
            pltpu.VMEM((1, value_size), jnp.float32),
            pltpu.VMEM((pieces, 4, width, span), jnp.bfloat16),
            pltpu.VMEM(output_weight.shape, jnp.bfloat16),
            pltpu.VMEM((pieces, seqs, span), jnp.float32),
            pltpu.VMEM((pieces, seqs, span), jnp.float32),
            pltpu.VMEM((rows, width), jnp.bfloat16),
            pltpu.VMEM((pieces, blocks, seqs, extent), jnp.bfloat16),
            pltpu.VMEM((pieces, chips, seqs, extent), jnp.bfloat16),
            pltpu.VMEM((pieces, chips, seqs, extent), jnp.bfloat16),
            pltpu.VMEM((pieces, chips + 1, seqs, extent), jnp.bfloat16),
            pltpu.VMEM((seqs, extent), jnp.float32),
            pltpu.VMEM((seqs, LANES), jnp.float32),
            pltpu.VMEM((16, 8 * LANES), jnp.bfloat16),
            pltpu.VMEM((seqs, span), jnp.float32),
            pltpu.VMEM((seqs, span), jnp.float32),
            pltpu.VMEM((pieces, seqs, span), jnp.bfloat16),
            pltpu.VMEM((pieces, blocks, seqs, span), jnp.bfloat16),
            pltpu.VMEM((rows, width), jnp.float32),
            dma((4,)),
            dma((pieces, 4)),
            dma,
            dma((pieces,)),
            dma((pieces, chips)),
            dma((pieces, chips)),
            dma((pieces, chips)),
            dma((pieces, chips + 1)),
            dma((pieces, chips)),
            dma((pieces, chips)),
            dma((pieces, blocks)),
        ],
        compiler_params=pltpu.CompilerParams(
            collective_id=collective_id, has_side_effects=True, vmem_limit_bytes=MIXER_LIMIT
        ),
    )(
        own,
        gain.reshape(blocks, 1, width),
        floor.reshape(pieces, 1, span),
        head_gain.reshape(1, value_size),
        *weights,
        output_weight,
        carried,
    )


def write_kernel(state, new_hbm, sem):
    rows = state.shape[0]
    chunks = sem.shape[0]
    size = rows // chunks

    def write_copy(i):
        at = pl.ds(i * size, size)
        return pltpu.make_async_copy(state.at[at], new_hbm.at[at], sem.at[i])

    @pl.loop(0, chunks)
    def _(i):
        write_copy(i).start()

    @pl.loop(0, chunks)
    def _(i):
        write_copy(i).wait()


def write_state(state):
    return pl.pallas_call(
        write_kernel,
        out_shape=jax.ShapeDtypeStruct(state.shape, jnp.float32),
        in_specs=[pl.BlockSpec(memory_space=pltpu.VMEM)],
        out_specs=pl.BlockSpec(memory_space=pl.ANY),
        scratch_shapes=[pltpu.SemaphoreType.DMA((8,))],
        compiler_params=pltpu.CompilerParams(vmem_limit_bytes=4 * 1024 * 1024),
    )(state)


def per_device(
    tokens,
    carried_state,
    first_gain,
    first_gate,
    first_up,
    first_down,
    mix_gain,
    query_weight,
    forget_weight,
    input_weight,
    outgate_weight,
    forget_floor,
    head_gain,
    output_weight,
    second_gain,
    second_gate,
    second_up,
    second_down,
):
    chips = lax.axis_size("kv")
    mixer_share = feed_forward(tokens, first_gain, first_gate, first_up, first_down, chips, 0)
    middle, held_state = mixer(
        mixer_share,
        mix_gain,
        (query_weight, forget_weight, input_weight, outgate_weight),
        output_weight,
        carried_state,
        forget_floor,
        head_gain,
        chips,
        1,
    )
    next_state = write_state(held_state)
    middle, next_state = lax.optimization_barrier((middle, next_state))
    layer_out = feed_forward(middle, second_gain, second_gate, second_up, second_down, chips, 2)
    return (layer_out, next_state)


def solution(mesh):
    in_specs = (
        P("dp", ("kv", "tp")),
        P(("dp", "kv", "tp"), None, None, None),
        P(),
        P(None, ("kv", "tp")),
        P(None, ("kv", "tp")),
        P(("kv", "tp"), None),
        P(),
        P(("kv", "tp"), None),
        P(("kv", "tp"), None),
        P(("kv", "tp"), None),
        P(("kv", "tp"), None),
        P(),
        P(),
        P(None, ("kv", "tp")),
        P(),
        P(None, ("kv", "tp")),
        P(None, ("kv", "tp")),
        P(("kv", "tp"), None),
    )
    out_specs = (P("dp", ("kv", "tp")), P(("dp", "kv", "tp"), None, None, None))
    return jax.shard_map(
        per_device, mesh=mesh, in_specs=in_specs, out_specs=out_specs, check_vma=False
    )
```
